32 devices in a mesh: grp: 2 (over y), sp: 4 (over z), tp: 4 (over x, core).
Axes of the slice: x: 2, y: 2, z: 4, core: 2. Of those that a mesh axis runs over, the one named last changes fastest.
Arguments:
- queries_small: bfloat16 [2048, 1024], P(('grp', 'sp'), 'tp'), parts along dimension 0, may hold values from -6 to 6
- keys_small: bfloat16 [2048, 512], P(('grp', 'sp'), 'tp'), parts along dimension 0, may hold values from -6 to 6
- values_small: bfloat16 [2048, 512], P(('grp', 'sp'), 'tp'), parts along dimension 0, may hold values from -6 to 6
- queries_large: bfloat16 [2048, 1024], P(('grp', 'sp'), 'tp'), parts along dimension 0, may hold values from -6 to 6
- keys_large: bfloat16 [2048, 512], P(('grp', 'sp'), 'tp'), parts along dimension 0, may hold values from -6 to 6
- values_large: bfloat16 [2048, 512], P(('grp', 'sp'), 'tp'), parts along dimension 0, may hold values from -6 to 6
- query_gain_small: float32 [128], P('grp'), parts along dimension 0, may hold values from 1.2 to 12
- key_gain_small: float32 [128], P('grp'), parts along dimension 0, may hold values from 1.2 to 12
- query_gain_large: float32 [256], P('grp'), parts along dimension 0, may hold values from 1.2 to 12
- key_gain_large: float32 [256], P('grp'), parts along dimension 0, may hold values from 1.2 to 12
- residual_in: bfloat16 [2048, 2048], P(('grp', 'sp', 'tp')), parts along dimension 0, may hold values from -1.5 to 1.5
- out_weight_small: bfloat16 [1024, 2048], P('tp'), may hold values from -0.125 to 0.125
- out_weight_large: bfloat16 [1024, 2048], P('tp'), may hold values from -0.125 to 0.125
- norm_gain: float32 [2048], replicated, may hold values from 0.1 to 1.9
- routes: int32 [2048, 2], P(('grp', 'sp', 'tp')), parts along dimension 0, may hold values from 0 to 7, all different within a row; in each aligned block of 64 rows (0 to 63, 64 to 127, ...) at most 32 rows name the same one
- route_scores: float32 [2048, 2], P(('grp', 'sp', 'tp')), parts along dimension 0, may hold values from 0.05 to 1
- expert_gate: bfloat16 [8, 2048, 1024], P('sp', None, 'tp'), may hold values from -0.125 to 0.125
- expert_up: bfloat16 [8, 2048, 1024], P('sp', None, 'tp'), may hold values from -0.125 to 0.125
- expert_down: bfloat16 [8, 1024, 2048], P('sp', 'tp'), may hold values from -0.1875 to 0.1875
Outputs:
- result: bfloat16 [2048, 2048], P(('grp', 'sp', 'tp')), parts along dimension 0
The draws below stay inside these ranges and needn't reach their ends.
There are 2 independent parts, one for each index of `grp`. The reference program is written for one: setup_inputs(seed, part) draws one part's arguments, and reference() takes and returns one part's arrays. A program takes and returns all parts, laid end to end along the dimension named above; an argument that names none is the same for every part. Nothing has to cross between parts.
Inputs may be any that keep to these rules, and one draw needn't show every extreme that they name: `routes`: each token names 2 different experts; within the rows of one device (aligned blocks of 64 tokens) no expert is named more than 32 times, a bound that some block reaches.
All inputs are finite; a program needn't handle non-finite values.
Results may differ from the reference program's by a relative error of at most 0.02.
The reference program's roundings to bfloat16 on the way count: a program that leaves them out, or rounds other values in their place, can miss the bound.
Values may be sent and summed in bfloat16 or wider, within the bound.
A program may use at most 128 MiB of HBM per device.

```python
import math
import jax
import jax.numpy as jnp
import numpy as np
from jax import lax

D = 2048
FFE = 1024
HS_SMALL = 64
HS_LARGE = 128
Q_SMALL = 16
KV_SMALL = 8
Q_LARGE = 8
KV_LARGE = 4
GRID_W = 64
TOP = 2
TOK_DEV = 256
SEQ = 1024
ROWS_DEV = 64
EXPERTS = 8
CAP = 32
N_TP = 4


def group_draw(key, query_heads, key_heads, head_size):
    draw_keys = jax.random.split(jax.random.fold_in(key, 7919 + head_size), 4)
    key_rows = jnp.clip(jax.random.normal(draw_keys[0], (SEQ, key_heads * head_size), jnp.float32), -6.0, 6.0)
    query_rows = jnp.clip(jax.random.normal(draw_keys[1], (SEQ, query_heads * head_size), jnp.float32), -6.0, 6.0)
    query_gain = jax.random.uniform(draw_keys[2], (head_size,), jnp.float32, 1.2, 2.0)
    key_gain = jax.random.uniform(draw_keys[3], (head_size,), jnp.float32, 1.2, 2.0)
    return (query_rows, key_rows, query_gain, key_gain)


def draw_queries_small(key, part):
    return group_draw(key, Q_SMALL, KV_SMALL, HS_SMALL)[0].astype(jnp.bfloat16)


def draw_keys_small(key, part):
    return group_draw(key, Q_SMALL, KV_SMALL, HS_SMALL)[1].astype(jnp.bfloat16)


def draw_query_gain_small(key, part):
    return group_draw(key, Q_SMALL, KV_SMALL, HS_SMALL)[2].astype(jnp.float32)


def draw_key_gain_small(key, part):
    return group_draw(key, Q_SMALL, KV_SMALL, HS_SMALL)[3].astype(jnp.float32)


def draw_queries_large(key, part):
    return group_draw(key, Q_LARGE, KV_LARGE, HS_LARGE)[0].astype(jnp.bfloat16)


def draw_keys_large(key, part):
    return group_draw(key, Q_LARGE, KV_LARGE, HS_LARGE)[1].astype(jnp.bfloat16)


def draw_query_gain_large(key, part):
    return group_draw(key, Q_LARGE, KV_LARGE, HS_LARGE)[2].astype(jnp.float32)


def draw_key_gain_large(key, part):
    return group_draw(key, Q_LARGE, KV_LARGE, HS_LARGE)[3].astype(jnp.float32)


def shard_levels(key, shape, pieces, low, largest):
    def one(axis_at, blocks):
        steps = jax.random.uniform(jax.random.fold_in(jax.random.fold_in(key, 6), axis_at), (blocks,), jnp.float32, low / len(pieces), largest / len(pieces))
        return jnp.repeat(jnp.exp(steps), shape[axis_at] // blocks).reshape((-1,) + (1,) * (len(shape) - axis_at - 1))

    loudness = one(*pieces[0])
    for cut in pieces[1:]:
        loudness = loudness * one(*cut)
    return loudness


def deal_out(own_key, own, number, rows, count, top, reach, slope):
    ranking = jax.random.permutation(own_key, count)
    crowded, usual = portions_of(count, rows * top, reach, slope, True), portions_of(count, rows * top, reach, slope, False)
    places = jnp.arange(count)

    def named(lengths, offset_by):
        used = int((lengths > 0).sum())
        fixed = max(1, used // 4)
        passed = fixed + (places - fixed + offset_by * (used - fixed)) % max(1, count - fixed)
        return jnp.zeros((count,), jnp.int32).at[ranking[jnp.where(places < fixed, places, passed)]].set(jnp.asarray(lengths, jnp.int32))

    lengths = jnp.where(number % 4 == 0, named(crowded, number // 4), named(usual, number - number // 4 - 1))
    mixed = jax.random.permutation(jax.random.fold_in(own, 3), count)
    giver, sink = mixed[0:count // 2 * 2:2], mixed[1:count // 2 * 2:2]
    slack = jnp.minimum(lengths[giver] - 1, reach - lengths[sink]) // 2
    slack = jnp.where((giver == ranking[0]) | (sink == ranking[0]) | (lengths[sink] == 0), 0, jnp.maximum(slack, 0))
    passed = jax.random.randint(jax.random.fold_in(own, 4), (count // 2,), 0, 1 << 20) % (slack + 1)
    lengths = lengths.at[giver].add(-passed).at[sink].add(passed)
    members = jnp.searchsorted(jnp.cumsum(lengths), jnp.arange(rows * top), side="right").astype(jnp.int32)
    listing = members.reshape(top, rows).T
    listing = listing[jax.random.permutation(jax.random.fold_in(own, 1), rows)]
    offset_by = jax.random.randint(jax.random.fold_in(own, 2), (rows, 1), 0, top)
    return jnp.take_along_axis(listing, (jnp.arange(top)[None, :] + offset_by) % top, axis=1)


def portions_of(amount, total, reach, skew, full):
    weights = [(1 << 20) // math.isqrt(standing ** skew) + 1 for standing in range(1, amount + 1)]
    largest = reach if full else min(reach, max(-(-total // amount), total * weights[0] // sum(weights)))
    least = 1 if total - largest >= amount - 1 else 0
    given, surplus = [largest] + [least] * (amount - 1), total - largest - least * (amount - 1)
    while surplus > 0:
        movable = [i for i in range(1, amount) if given[i] < largest] or [i for i in range(1, amount) if given[i] < reach]
        mass, remaining = sum([weights[i] for i in movable]), surplus
        for i in movable:
            addition = min(reach - given[i], max(1, remaining * weights[i] // mass), surplus)
            given[i] = given[i] + addition
            surplus = surplus - addition
    return np.array(given)


def normal_values(key, extent, scale, most, cuts=(), held_as=jnp.bfloat16):
    factor_of = shard_levels(key, extent, cuts, -0.22, 0.18) if cuts else 1.0
    array = jax.random.normal(key, extent, jnp.float32) * scale * factor_of
    return jnp.minimum(jnp.maximum(array, -most), most).astype(held_as)


def setup_inputs(seed: int = 0, part: int = 0) -> dict:
    keys = jax.random.split(jax.random.key(seed), 20)
    part_keys = jax.random.split(jax.random.fold_in(keys[19], part), 20)
    queries_small = draw_queries_small(jax.random.fold_in(jax.random.fold_in(keys[19], part), 71), part)
    keys_small = draw_keys_small(jax.random.fold_in(jax.random.fold_in(keys[19], part), 71), part)
    values_small = normal_values(part_keys[2], (SEQ, KV_SMALL * HS_SMALL), 1.0, 6.0, ((0, 4), (1, 4)))
    queries_large = draw_queries_large(jax.random.fold_in(jax.random.fold_in(keys[19], part), 71), part)
    keys_large = draw_keys_large(jax.random.fold_in(jax.random.fold_in(keys[19], part), 71), part)
    values_large = normal_values(part_keys[5], (SEQ, KV_LARGE * HS_LARGE), 1.0, 6.0, ((0, 4), (1, 4)))
    query_gain_small = draw_query_gain_small(jax.random.fold_in(jax.random.fold_in(keys[19], part), 71), part)
    key_gain_small = draw_key_gain_small(jax.random.fold_in(jax.random.fold_in(keys[19], part), 71), part)
    query_gain_large = draw_query_gain_large(jax.random.fold_in(jax.random.fold_in(keys[19], part), 71), part)
    key_gain_large = draw_key_gain_large(jax.random.fold_in(jax.random.fold_in(keys[19], part), 71), part)
    residual_in = normal_values(part_keys[10], (SEQ, D), 0.25, 1.5, ((0, 16),))
    out_weight_small = normal_values(keys[11], (Q_SMALL * HS_SMALL, D), (Q_SMALL * HS_SMALL + Q_LARGE * HS_LARGE) ** -0.5, 0.125, ((0, 4),))
    out_weight_large = normal_values(keys[12], (Q_LARGE * HS_LARGE, D), (Q_SMALL * HS_SMALL + Q_LARGE * HS_LARGE) ** -0.5, 0.125, ((0, 4),))
    norm_gain = jnp.clip(1.0 + 0.18 * jax.random.normal(keys[13], (D,), jnp.float32), 0.1, 1.9)
    routes_keys = jax.random.split(jax.random.fold_in(part_keys[14], 1), SEQ // ROWS_DEV)
    routes_turns = jax.random.permutation(jax.random.fold_in(part_keys[14], 3), SEQ // ROWS_DEV)
    routes = jax.vmap(lambda own, number: deal_out(jax.random.fold_in(part_keys[14], 2), own, number, ROWS_DEV, EXPERTS, TOP, CAP, 1))(routes_keys, routes_turns).reshape((SEQ, TOP))
    route_scores = jnp.clip(0.05 + 0.95 * jax.random.uniform(part_keys[15], (SEQ, TOP), jnp.float32) ** shard_levels(part_keys[15], (SEQ, TOP), ((0, 16),), -0.2, 0.2), 0.05, 1.0)
    expert_gate = normal_values(keys[16], (EXPERTS, D, FFE), D ** -0.5, 0.125, ((0, 4), (2, 4)))
    expert_up = normal_values(keys[17], (EXPERTS, D, FFE), D ** -0.5, 0.125, ((0, 4), (2, 4)))
    expert_down = normal_values(keys[18], (EXPERTS, FFE, D), FFE ** -0.5, 0.1875, ((0, 4), (1, 4)))
    return dict(queries_small=queries_small, keys_small=keys_small, values_small=values_small, queries_large=queries_large, keys_large=keys_large, values_large=values_large, query_gain_small=query_gain_small, key_gain_small=key_gain_small, query_gain_large=query_gain_large, key_gain_large=key_gain_large, residual_in=residual_in, out_weight_small=out_weight_small, out_weight_large=out_weight_large, norm_gain=norm_gain, routes=routes, route_scores=route_scores, expert_gate=expert_gate, expert_up=expert_up, expert_down=expert_down)


theta_base = 10000.0
norm_eps = 1e-06

def grid_tables(offset, length, head_size):
    places = offset + jnp.arange(length, dtype=jnp.int32)
    grid_rows = (places // GRID_W).astype(jnp.float32)
    grid_cols = (places % GRID_W).astype(jnp.float32)
    rates = jnp.power(theta_base, -2.0 * jnp.arange(head_size // 4, dtype=jnp.float32) / (head_size // 2))
    row_angles = grid_rows[:, None, None] * rates
    col_angles = grid_cols[:, None, None] * rates
    return (jnp.cos(row_angles), jnp.sin(row_angles), jnp.cos(col_angles), jnp.sin(col_angles))

def half_turn(segment, cosine, sine_part):
    half_size = segment.shape[-1] // 2
    leading = segment[..., :half_size]
    trailing = segment[..., half_size:]
    return jnp.concatenate([leading * cosine - trailing * sine_part, trailing * cosine + leading * sine_part], axis=-1)

def grid_turn(vectors, tables):
    row_cos, row_sin, col_cos, col_sin = tables
    half_size = vectors.shape[-1] // 2
    return jnp.concatenate([half_turn(vectors[..., :half_size], row_cos, row_sin), half_turn(vectors[..., half_size:], col_cos, col_sin)], axis=-1)

def normed_turn(raw_rows, gain, tables):
    widened = raw_rows.astype(jnp.float32)
    scaled = widened * lax.rsqrt(lax.optimization_barrier(jnp.mean(widened * widened, axis=-1, keepdims=True)) + norm_eps) * gain
    return grid_turn(scaled, tables).astype(jnp.bfloat16)

def attend_group(queries, key_rows, value_rows, query_gain, key_gain, head_size):
    seq_len = queries.shape[0]
    query_heads = queries.shape[1] // head_size
    key_heads = key_rows.shape[1] // head_size
    group_ratio = query_heads // key_heads
    tables = grid_tables(0, seq_len, head_size)
    asked = normed_turn(queries.reshape(seq_len, query_heads, head_size), query_gain, tables)
    keyed = normed_turn(key_rows.reshape(seq_len, key_heads, head_size), key_gain, tables)
    valued = value_rows.reshape(seq_len, key_heads, head_size)

    def one_head(head_index):
        asked_head = lax.dynamic_index_in_dim(asked, head_index, 1, keepdims=False)
        keyed_head = lax.dynamic_index_in_dim(keyed, head_index // group_ratio, 1, keepdims=False)
        valued_head = lax.dynamic_index_in_dim(valued, head_index // group_ratio, 1, keepdims=False)

        def one_block(query_block):
            scores = jnp.dot(query_block, keyed_head.T, preferred_element_type=jnp.float32) * head_size ** (-0.5)
            peak_score = lax.optimization_barrier(jnp.max(scores, axis=1, keepdims=True))
            weights = jnp.exp(scores - peak_score)
            summed = jnp.dot(weights.astype(jnp.bfloat16), valued_head, preferred_element_type=jnp.float32)
            return (summed / lax.optimization_barrier(jnp.sum(weights, axis=1, keepdims=True))).astype(jnp.bfloat16)
        blocks = asked_head.reshape(seq_len // TOK_DEV, TOK_DEV, head_size)
        return lax.map(one_block, blocks).reshape(seq_len, head_size)
    heard = lax.map(one_head, jnp.arange(query_heads, dtype=jnp.int32))
    return jnp.transpose(heard, (1, 0, 2)).reshape(seq_len, query_heads * head_size)

def expert_chain(rows_in, gate_weight, up_weight, down_weight):
    gate_out = jnp.dot(rows_in, gate_weight, preferred_element_type=jnp.float32)
    up_out = jnp.dot(rows_in, up_weight, preferred_element_type=jnp.float32)
    active = (jax.nn.silu(gate_out) * up_out).astype(jnp.bfloat16)
    width_part = FFE // N_TP
    total_terms = jnp.zeros((rows_in.shape[0], D), jnp.float32)
    for part_index in range(N_TP):
        lower = part_index * width_part
        term = jnp.dot(active[:, lower:lower + width_part], down_weight[lower:lower + width_part], preferred_element_type=jnp.float32).astype(jnp.bfloat16)
        total_terms = total_terms + lax.optimization_barrier(term).astype(jnp.float32)
    return total_terms.astype(jnp.bfloat16)

def reference(queries_small, keys_small, values_small, queries_large, keys_large, values_large, query_gain_small, key_gain_small, query_gain_large, key_gain_large, residual_in, out_weight_small, out_weight_large, norm_gain, routes, route_scores, expert_gate, expert_up, expert_down):
    heard_small = attend_group(queries_small, keys_small, values_small, query_gain_small, key_gain_small, HS_SMALL)
    heard_large = attend_group(queries_large, keys_large, values_large, query_gain_large, key_gain_large, HS_LARGE)
    small_cols = Q_SMALL * HS_SMALL // N_TP
    large_cols = Q_LARGE * HS_LARGE // N_TP
    projected = jnp.zeros((SEQ, D), jnp.float32)
    for part_index in range(N_TP):
        lower_small = part_index * small_cols
        lower_large = part_index * large_cols
        term = jnp.dot(heard_small[:, lower_small:lower_small + small_cols], out_weight_small[lower_small:lower_small + small_cols], preferred_element_type=jnp.float32) + jnp.dot(heard_large[:, lower_large:lower_large + large_cols], out_weight_large[lower_large:lower_large + large_cols], preferred_element_type=jnp.float32)
        term = term.astype(jnp.bfloat16)
        projected = projected + lax.optimization_barrier(term).astype(jnp.float32)
    attended = (residual_in.astype(jnp.float32) + projected).astype(jnp.bfloat16)
    widened = attended.astype(jnp.float32)
    normed = (widened * lax.rsqrt(lax.optimization_barrier(jnp.mean(widened * widened, axis=-1, keepdims=True)) + norm_eps) * norm_gain).astype(jnp.bfloat16)
    shares = route_scores / lax.optimization_barrier(jnp.sum(route_scores, axis=1, keepdims=True))
    block_count = SEQ // ROWS_DEV
    flat_routes = routes.reshape(block_count, ROWS_DEV * TOP)
    member = (flat_routes[:, :, None] == jnp.arange(EXPERTS, dtype=jnp.int32)[None, None, :]).astype(jnp.int32)
    ranks = lax.optimization_barrier(jnp.sum((jnp.cumsum(member, axis=1) - member) * member, axis=2))
    slot_within = jnp.arange(block_count, dtype=jnp.int32)[:, None] * CAP + ranks
    token_ids = jnp.arange(SEQ, dtype=jnp.int32).reshape(block_count, ROWS_DEV)
    token_of = jnp.broadcast_to(token_ids[:, :, None], (block_count, ROWS_DEV, TOP)).reshape(-1)
    slot_tokens = jnp.zeros((EXPERTS, block_count * CAP), jnp.int32).at[flat_routes.reshape(-1), slot_within.reshape(-1)].set(token_of)
    slot_shares = jnp.zeros((EXPERTS, block_count * CAP), jnp.float32).at[flat_routes.reshape(-1), slot_within.reshape(-1)].set(shares.reshape(-1))

    def add_expert(mixed, inputs):
        tokens_here, shares_here, gate_weight, up_weight, down_weight = inputs
        outputs = expert_chain(normed[tokens_here], gate_weight, up_weight, down_weight)
        return (mixed.at[tokens_here].add(outputs.astype(jnp.float32) * shares_here[:, None]), None)
    mixed = lax.scan(add_expert, jnp.zeros((SEQ, D), jnp.float32), (slot_tokens, slot_shares, expert_gate, expert_up, expert_down))[0]
    return (attended.astype(jnp.float32) + mixed).astype(jnp.bfloat16)
```

```python
import functools

import jax
import jax.numpy as jnp
import numpy as np
from jax import lax
from jax.experimental import pallas as pl
from jax.experimental.pallas import tpu as pltpu
from jax.sharding import PartitionSpec as P

HS_SMALL = 64
HS_LARGE = 128
GRID_W = 64


theta_base = 10000.0
norm_eps = 1e-06
block_target = 1280


def grid_tables(offset, length, head_size):
    places = offset + jnp.arange(length, dtype=jnp.int32)
    grid_rows = (places // GRID_W).astype(jnp.float32)
    grid_cols = (places % GRID_W).astype(jnp.float32)
    rates = jnp.power(
        theta_base, -2.0 * jnp.arange(head_size // 4, dtype=jnp.float32) / (head_size // 2)
    )
    row_angles = grid_rows[:, None, None] * rates
    col_angles = grid_cols[:, None, None] * rates
    return (jnp.cos(row_angles), jnp.sin(row_angles), jnp.cos(col_angles), jnp.sin(col_angles))


def half_turn(segment, cosine, sine_part):
    half_size = segment.shape[-1] // 2
    leading = segment[..., :half_size]
    trailing = segment[..., half_size:]
    return jnp.concatenate(
        [leading * cosine - trailing * sine_part, trailing * cosine + leading * sine_part], axis=-1
    )


def grid_turn(vectors, tables):
    row_cos, row_sin, col_cos, col_sin = tables
    half_size = vectors.shape[-1] // 2
    return jnp.concatenate(
        [
            half_turn(vectors[..., :half_size], row_cos, row_sin),
            half_turn(vectors[..., half_size:], col_cos, col_sin),
        ],
        axis=-1,
    )


def normed_turn(raw_rows, gain, tables):
    widened = raw_rows.astype(jnp.float32)
    scaled = (
        widened * lax.rsqrt(jnp.mean(widened * widened, axis=-1, keepdims=True) + norm_eps) * gain
    )
    return grid_turn(scaled, tables).astype(jnp.bfloat16)


def block_rows(row_count, shard_rows):
    shards = row_count // shard_rows
    chosen = 1
    for factor in range(1, max(1, block_target // shard_rows) + 1):
        if shards % factor == 0:
            chosen = factor
    return chosen * shard_rows


def attend_block(state, queries, key_rows, value_rows):
    largest, weight_sum, accumulated = state
    head_size = queries.shape[-1]
    kv_local = queries.shape[1]
    key_heads = key_rows.reshape(key_rows.shape[0], kv_local, head_size)
    value_heads = value_rows.reshape(value_rows.shape[0], kv_local, head_size)
    scores = jnp.einsum(
        "qgrd,kgd->qgrk", queries, key_heads, preferred_element_type=jnp.float32
    ) * head_size ** (-0.5)
    peak_score = jnp.maximum(largest, jnp.max(scores, axis=-1))
    shrink = jnp.exp(largest - peak_score)
    weights = jnp.exp(scores - peak_score[..., None])
    weight_sum = weight_sum * shrink + jnp.sum(weights, axis=-1)
    accumulated = accumulated * shrink[..., None] + jnp.einsum(
        "qgrk,kgd->qgrd",
        weights.astype(jnp.bfloat16),
        value_heads,
        preferred_element_type=jnp.float32,
    )
    return (peak_score, weight_sum, accumulated)


def attend_rows(state, queries, key_rows, value_rows):
    row_count = key_rows.shape[0]
    step_rows = block_rows(row_count, queries.shape[0])
    if step_rows == row_count:
        return attend_block(state, queries, key_rows, value_rows)

    def one_block(block_index, carried):
        offset = block_index * step_rows
        return attend_block(
            carried,
            queries,
            lax.dynamic_slice_in_dim(key_rows, offset, step_rows, 0),
            lax.dynamic_slice_in_dim(value_rows, offset, step_rows, 0),
        )

    return lax.fori_loop(0, row_count // step_rows, one_block, state)


def empty_state(queries):
    state_shape = queries.shape[:3]
    return (
        jnp.full(state_shape, -1e30, jnp.float32),
        jnp.zeros(state_shape, jnp.float32),
        jnp.zeros(queries.shape, jnp.float32),
    )


def finish(state):
    largest, weight_sum, accumulated = state
    merged = accumulated / weight_sum[..., None]
    return merged.reshape(merged.shape[0], -1).astype(jnp.bfloat16)


def on_device(
    queries_small,
    keys_small,
    values_small,
    queries_large,
    keys_large,
    values_large,
    query_gain_small,
    key_gain_small,
    query_gain_large,
    key_gain_large,
    residual_in,
    out_weight_small,
    out_weight_large,
    norm_gain,
    routes,
    route_scores,
    expert_gate,
    expert_up,
    expert_down,
):
    token_rows = queries_small.shape[0]
    offset = lax.axis_index("sp") * token_rows
    tables_small = grid_tables(offset, token_rows, HS_SMALL)
    tables_large = grid_tables(offset, token_rows, HS_LARGE)
    kv_small = keys_small.shape[1] // HS_SMALL
    kv_large = keys_large.shape[1] // HS_LARGE
    asked_small = normed_turn(
        queries_small.reshape(token_rows, -1, HS_SMALL), query_gain_small, tables_small
    ).reshape(token_rows, kv_small, -1, HS_SMALL)
    asked_large = normed_turn(
        queries_large.reshape(token_rows, -1, HS_LARGE), query_gain_large, tables_large
    ).reshape(token_rows, kv_large, -1, HS_LARGE)
    turned_small = normed_turn(
        keys_small.reshape(token_rows, kv_small, HS_SMALL), key_gain_small, tables_small
    ).reshape(token_rows, -1)
    turned_large = normed_turn(
        keys_large.reshape(token_rows, kv_large, HS_LARGE), key_gain_large, tables_large
    ).reshape(token_rows, -1)
    key_small = lax.all_gather(turned_small, "sp", axis=0, tiled=True)
    value_small = lax.all_gather(values_small, "sp", axis=0, tiled=True)
    key_large = lax.all_gather(turned_large, "sp", axis=0, tiled=True)
    value_large = lax.all_gather(values_large, "sp", axis=0, tiled=True)
    state_small = attend_rows(empty_state(asked_small), asked_small, key_small, value_small)
    state_large = attend_rows(empty_state(asked_large), asked_large, key_large, value_large)
    heard_small = finish(state_small)
    heard_large = finish(state_large)
    projected = lax.psum_scatter(
        (
            jnp.dot(heard_small, out_weight_small, preferred_element_type=jnp.float32)
            + jnp.dot(heard_large, out_weight_large, preferred_element_type=jnp.float32)
        ).astype(jnp.bfloat16),
        "tp",
        scatter_dimension=0,
        tiled=True,
    ).astype(jnp.float32)
    attended = (residual_in.astype(jnp.float32) + projected).astype(jnp.bfloat16)
    widened = attended.astype(jnp.float32)
    normed = (
        widened
        * lax.rsqrt(jnp.mean(widened * widened, axis=-1, keepdims=True) + norm_eps)
        * norm_gain
    ).astype(jnp.bfloat16)
    local_rows = routes.shape[0]
    top_count = routes.shape[1]
    sp_count = lax.axis_size("sp")
    local_experts = expert_gate.shape[0]
    expert_count = local_experts * sp_count
    capacity = max(2, (2 * top_count * local_rows + expert_count - 1) // expert_count)
    flat_routes = routes.reshape(-1)
    member = (flat_routes[:, None] == jnp.arange(expert_count, dtype=jnp.int32)[None, :]).astype(
        jnp.int32
    )
    ranks = jnp.sum((jnp.cumsum(member, axis=0) - member) * member, axis=1)
    slots = flat_routes * capacity + ranks
    picker = (
        slots[:, None] == jnp.arange(expert_count * capacity, dtype=jnp.int32)[None, :]
    ).astype(jnp.bfloat16)
    placer = jnp.sum(picker.reshape(local_rows, top_count, -1), axis=1)
    outgoing = jnp.einsum("ts,td->sd", placer, normed, preferred_element_type=jnp.float32).astype(
        jnp.bfloat16
    )
    outgoing = outgoing.reshape(sp_count, local_experts, capacity, -1)
    everyone = lax.all_gather(
        lax.all_to_all(outgoing, "sp", split_axis=0, concat_axis=0, tiled=True),
        "tp",
        axis=0,
        tiled=True,
    )
    gate_out = jnp.einsum(
        "secd,edf->secf", everyone, expert_gate, preferred_element_type=jnp.float32
    )
    up_out = jnp.einsum("secd,edf->secf", everyone, expert_up, preferred_element_type=jnp.float32)
    active = (jax.nn.silu(gate_out) * up_out).astype(jnp.bfloat16)
    summed = lax.psum_scatter(
        jnp.einsum(
            "secf,efd->secd", active, expert_down, preferred_element_type=jnp.float32
        ).astype(jnp.bfloat16),
        "tp",
        scatter_dimension=0,
        tiled=True,
    )
    returned = lax.all_to_all(summed, "sp", split_axis=0, concat_axis=0, tiled=True)
    back_rows = returned.reshape(expert_count * capacity, -1)
    chosen_rows = jnp.dot(picker, back_rows, preferred_element_type=jnp.float32).reshape(
        local_rows, top_count, -1
    )
    shares = route_scores / jnp.sum(route_scores, axis=1, keepdims=True)
    mixed = jnp.sum(chosen_rows * shares[:, :, None], axis=1)
    return (attended.astype(jnp.float32) + mixed).astype(jnp.bfloat16)


MESH = pl.DeviceIdType.MESH
LANES = 128


def rotary_tables(grid_rows, head_size):
    lane = np.arange(LANES) % head_size
    rates = np.power(
        np.float32(theta_base),
        (np.float32(-2.0) * np.arange(head_size // 4, dtype=np.float32) / np.float32(head_size // 2)),
    ).astype(np.float32)
    rate = rates[lane % (head_size // 4)]
    is_row = lane < head_size // 2
    sign = np.where(lane % (head_size // 2) < head_size // 4, -1.0, 1.0)

    def build(count, keep):
        angles = np.arange(count, dtype=np.float32)[:, None] * rate[None, :]
        angles = angles.astype(np.float64)
        return (
            np.where(keep, np.cos(angles), 0.0).astype(np.float32),
            np.where(keep, np.sin(angles) * sign, 0.0).astype(np.float32),
        )

    return build(grid_rows, is_row), build(GRID_W, ~is_row)


def visit_order(count):
    return [sorted(range(count), key=lambda b: (abs(b - at), b)) for at in range(count)]


def pick(table, at, step):
    chosen = jnp.int32(0)
    for i, row in enumerate(table):
        for j, entry in enumerate(row):
            chosen = jnp.where((at == i) & (step == j), jnp.int32(entry), chosen)
    return chosen


def lanes_of(shape):
    return lax.broadcasted_iota(jnp.int32, shape, len(shape) - 1)


def turn_rows(raw, gain, cosine, sine, head_size):
    wide = raw.astype(jnp.float32)
    lane = lanes_of(wide.shape)
    squares = wide * wide
    if head_size == LANES:
        scale = lax.rsqrt(jnp.sum(squares, axis=-1, keepdims=True) / head_size + norm_eps)
    else:
        low = lane < head_size
        first = jnp.sum(jnp.where(low, squares, 0.0), axis=-1, keepdims=True) / head_size
        second = jnp.sum(jnp.where(low, 0.0, squares), axis=-1, keepdims=True) / head_size
        scale = jnp.where(low, lax.rsqrt(first + norm_eps), lax.rsqrt(second + norm_eps))
    scaled = wide * scale * gain
    quarter = head_size // 4
    ahead = pltpu.roll(scaled, LANES - quarter, 1)
    behind = pltpu.roll(scaled, quarter, 1)
    partner = jnp.where(lane % (2 * quarter) < quarter, ahead, behind)
    return scaled * cosine + partner * sine


def layer_kernel(
    sp_count,
    q_s, k_s, v_s, q_l, k_l, v_l, gains, row_tab, col_tab, residual, norm_gain, routes, scores,
    ws_any, wl_any, eg_any, eu_any, ed_any,
    out,
    kv, qst, big, den, acc, heard, w_out, w_gate, w_up, w_down,
    p_out, p_in, x_out, x_in, att, ag,
    y_out, y_in, s1, xs, rx, zs, rz,
    w_sem, kv_send, kv_recv, p_send, p_recv, ag_send, ag_fwd, ag_recv,
    yc_send, yc_recv, rx_send, rx_recv, rz_send, rz_recv,
):
    n = sp_count
    z = lax.axis_index("sp")
    tp = lax.axis_index("tp")
    x, c = tp // 2, tp % 2
    sibling = {"tp": x * 2 + (1 - c)}
    across = {"tp": (1 - x) * 2 + c}
    order = visit_order(n)
    tokens = q_s.shape[0]
    rows = residual.shape[0]
    width = residual.shape[1]
    experts_here = eg_any.shape[0]
    hidden = eg_any.shape[2]

    def remote(src, dst, send, recv, to):
        return pltpu.make_async_remote_copy(
            src_ref=src, dst_ref=dst, send_sem=send, recv_sem=recv, device_id=to, device_id_type=MESH
        )

    half = ws_any.shape[0]
    loads = [
        pltpu.make_async_copy(ws_any, w_out.at[pl.ds(0, half)], w_sem.at[0]),
        pltpu.make_async_copy(wl_any, w_out.at[pl.ds(half, half)], w_sem.at[1]),
        pltpu.make_async_copy(eg_any, w_gate, w_sem.at[2]),
        pltpu.make_async_copy(eu_any, w_up, w_sem.at[3]),
        pltpu.make_async_copy(ed_any, w_down, w_sem.at[4]),
    ]
    for load in loads:
        load.start()

    barrier = pltpu.get_barrier_semaphore()
    for away in range(1, n):
        pl.semaphore_signal(barrier, inc=1, device_id={"sp": (z + away) % n}, device_id_type=MESH)
    pl.semaphore_signal(barrier, inc=1, device_id=sibling, device_id_type=MESH)
    pl.semaphore_signal(barrier, inc=1, device_id=across, device_id_type=MESH)

    strips = tokens // GRID_W

    def table(kind):
        pieces = [
            row_tab[kind, pl.ds(z * strips + r, 1), :] + col_tab[kind] for r in range(strips)
        ]
        return jnp.concatenate(pieces, axis=0)

    cos_s, sin_s, cos_l, sin_l = table(0), table(1), table(2), table(3)
    kv[z, 1] = v_s[...]
    kv[z, 3] = v_l[...]
    kv[z, 0] = turn_rows(k_s[...], gains[1:2, :], cos_s, sin_s, HS_SMALL).astype(jnp.bfloat16)
    kv[z, 2] = turn_rows(k_l[...], gains[3:4, :], cos_l, sin_l, HS_LARGE).astype(jnp.bfloat16)
    pl.semaphore_wait(barrier, n + 1)

    def kv_copy(b, d):
        return remote(
            kv.at[b], kv.at[b], kv_send.at[b, (d + 1) // 2], kv_recv.at[b], {"sp": z + d}
        )

    for d in (1, -1):
        @pl.when((z + d >= 0) & (z + d < n))
        def _():
            kv_copy(z, d).start()

    low = lanes_of((tokens, LANES)) < HS_SMALL
    zero = jnp.zeros((tokens, LANES), jnp.float32)
    q01 = turn_rows(q_s[:, :LANES], gains[0:1, :], cos_s, sin_s, HS_SMALL)
    q23 = turn_rows(q_s[:, LANES:], gains[0:1, :], cos_s, sin_s, HS_SMALL)
    qst[0, :tokens] = jnp.where(low, q01, zero).astype(jnp.bfloat16)
    qst[0, tokens:] = jnp.where(low, pltpu.roll(q01, HS_SMALL, 1), zero).astype(jnp.bfloat16)
    qst[1, :tokens] = jnp.where(low, zero, pltpu.roll(q23, HS_SMALL, 1)).astype(jnp.bfloat16)
    qst[1, tokens:] = jnp.where(low, zero, q23).astype(jnp.bfloat16)
    for h in range(2):
        piece = q_l[:, h * LANES : (h + 1) * LANES]
        qst[2, h * tokens : (h + 1) * tokens] = turn_rows(
            piece, gains[2:3, :], cos_l, sin_l, HS_LARGE
        ).astype(jnp.bfloat16)
    big[...] = jnp.full(big.shape, -1e30, jnp.float32)
    den[...] = jnp.zeros(den.shape, jnp.float32)
    acc[...] = jnp.zeros(acc.shape, jnp.float32)

    def attend(j, carry):
        b = pick(order, z, j)
        d = jnp.where(b < z, 1, -1)

        @pl.when(j > 0)
        def _():
            kv_copy(b, 1).wait_recv()

            for way in (1, -1):
                @pl.when((d == way) & (z + way >= 0) & (z + way < n))
                def _():
                    kv_copy(b, way).start()

        for g in range(3):
            keys = kv[b, 0 if g < 2 else 2]
            values = kv[b, 1 if g < 2 else 3]
            scale = (HS_SMALL if g < 2 else HS_LARGE) ** (-0.5)
            score = (
                lax.dot_general(
                    qst[g], keys, (((1,), (1,)), ((), ())), preferred_element_type=jnp.float32
                )
                * scale
            )
            before = big[g]
            peak = jnp.maximum(before, jnp.max(score, axis=-1, keepdims=True))
            shrink = jnp.exp(before - peak)
            weight = jnp.exp(score - peak[:, :1])
            den[g] = den[g] * shrink + jnp.sum(weight, axis=-1, keepdims=True)
            acc[g] = acc[g] * shrink + jnp.dot(
                weight.astype(jnp.bfloat16), values, preferred_element_type=jnp.float32
            )
            big[g] = peak
        return carry

    lax.fori_loop(0, n, attend, 0)

    o0, o1, o2 = acc[0] / den[0], acc[1] / den[1], acc[2] / den[2]
    heard[:, 0:LANES] = jnp.where(low, o0[:tokens], pltpu.roll(o0[tokens:], HS_SMALL, 1)).astype(
        jnp.bfloat16
    )
    heard[:, LANES : 2 * LANES] = jnp.where(
        low, pltpu.roll(o1[:tokens], HS_SMALL, 1), o1[tokens:]
    ).astype(jnp.bfloat16)
    heard[:, 2 * LANES : 3 * LANES] = o2[:tokens].astype(jnp.bfloat16)
    heard[:, 3 * LANES : 4 * LANES] = o2[tokens:].astype(jnp.bfloat16)

    loads[0].wait()
    loads[1].wait()

    def projected(core):
        lhs = jnp.concatenate(
            [heard[pl.ds((xx * 2 + core) * rows, rows), :] for xx in range(2)], axis=0
        )
        return jnp.dot(lhs, w_out[...], preferred_element_type=jnp.float32).astype(jnp.bfloat16)

    p_out[...] = projected(1 - c)
    to_sibling = remote(p_out, p_in, p_send.at[0], p_recv.at[0], sibling)
    to_sibling.start()
    own_term = projected(c).astype(jnp.float32)
    to_sibling.wait_recv()
    pair = own_term + p_in[...].astype(jnp.float32)
    here_first = x == 0
    x_out[...] = jnp.where(here_first, pair[rows:], pair[:rows]).astype(jnp.bfloat16)
    to_across = remote(x_out, x_in, p_send.at[1], p_recv.at[1], across)
    to_across.start()
    kept = jnp.where(here_first, pair[:rows], pair[rows:]) + residual[...].astype(jnp.float32)

    share = scores[...] / jnp.sum(scores[...], axis=1, keepdims=True)
    lane = lanes_of((rows, LANES))
    dense = jnp.zeros((rows, LANES), jnp.float32)
    for t in range(routes.shape[1]):
        dense = jnp.where(lane == routes[:, t : t + 1], share[:, t : t + 1], dense)
    dense_high = dense.astype(jnp.bfloat16).astype(jnp.float32)
    packed = dense_high + pltpu.roll(dense - dense_high, LANES // 2, 1)
    ag[z, x, c, :, width:] = packed.astype(jnp.bfloat16)

    to_across.wait_recv()
    attended = (kept + x_in[...].astype(jnp.float32)).astype(jnp.bfloat16)
    att[...] = attended
    wide = attended.astype(jnp.float32)
    ag[z, x, c, :, :width] = (
        wide
        * lax.rsqrt(jnp.sum(wide * wide, axis=-1, keepdims=True) / width + norm_eps)
        * norm_gain[...]
    ).astype(jnp.bfloat16)

    def ag_copy(b, xx, cc, sem, to):
        block = ag.at[b, xx, cc]
        return remote(block, block, sem, ag_recv.at[b, xx, cc], to)

    def line_copy(b, d):
        return ag_copy(b, x, c, ag_send.at[b, (d + 1) // 2], {"sp": z + d})

    def spread(b):
        return (
            ag_copy(b, x, c, ag_send.at[b, 2], across),
            ag_copy(b, x, c, ag_send.at[b, 3], sibling),
        )

    def forward(b):
        return ag_copy(b, 1 - x, c, ag_fwd.at[b], sibling)

    for d in (1, -1):
        @pl.when((z + d >= 0) & (z + d < n))
        def _():
            line_copy(z, d).start()

    for copy in spread(z):
        copy.start()

    def y_copy(b):
        return remote(y_out.at[b], y_in.at[b], yc_send.at[b], yc_recv.at[b], sibling)

    def x_copy(b):
        return remote(xs.at[b], rx.at[b], rx_send.at[b], rx_recv.at[b], across)

    def z_copy(b):
        return remote(zs.at[b], rz.at[z], rz_send.at[b], rz_recv.at[z], {"sp": b})

    def settle(b):
        x_copy(b).wait_recv()
        total = s1[b] + rx[b].astype(jnp.float32)

        @pl.when(b == z)
        def _():
            s1[b] = total

        @pl.when(b != z)
        def _():
            zs[b] = total.astype(jnp.bfloat16)
            z_copy(b).start()

    for load in loads[2:]:
        load.wait()

    def experts(j, carry):
        b = pick(order, z, j)

        @pl.when(j < n - 1)
        def _():
            later = pick(order, z, j + 1)
            ag_copy(later, x, c, ag_send.at[later, 2], across).wait_recv()
            for way in (1, -1):
                @pl.when((jnp.where(later < z, 1, -1) == way) & (z + way >= 0) & (z + way < n))
                def _():
                    line_copy(later, way).start()

            for copy in spread(later):
                copy.start()

        ag_copy(b, 1 - x, c, ag_fwd.at[b], sibling).wait_recv()
        forward(b).start()
        for xx in (x, 1 - x):
            ag_copy(b, xx, 1 - c, ag_fwd.at[b], sibling).wait_recv()
        blocks = [ag[b, xx, cc] for cc in (1 - c, c) for xx in range(2)]
        rows_in = jnp.concatenate([block[:, :width] for block in blocks], axis=0)
        marks = jnp.concatenate([block[:, width:] for block in blocks], axis=0).astype(jnp.float32)
        mark_lane = lanes_of(marks.shape) % (LANES // 2)
        active = []
        for e in range(experts_here):
            gate = jnp.dot(rows_in, w_gate[e], preferred_element_type=jnp.float32)
            up = jnp.dot(rows_in, w_up[e], preferred_element_type=jnp.float32)
            weight = jnp.sum(
                jnp.where(mark_lane == z * experts_here + e, marks, 0.0), axis=1, keepdims=True
            )
            active.append((gate / (1.0 + jnp.exp(-gate)) * up * weight).astype(jnp.bfloat16))
        hidden_rows = jnp.concatenate(active, axis=1)
        down = w_down[...].reshape(experts_here * hidden, width)
        split = 2 * rows
        y_out[b] = jnp.dot(
            hidden_rows[:split], down, preferred_element_type=jnp.float32
        ).astype(jnp.bfloat16)
        y_copy(b).start()
        mine = jnp.dot(hidden_rows[split:], down, preferred_element_type=jnp.float32)
        y_copy(b).wait_recv()
        both = mine + y_in[b].astype(jnp.float32)
        xs[b] = jnp.where(x == 0, both[rows:], both[:rows]).astype(jnp.bfloat16)
        x_copy(b).start()
        s1[b] = jnp.where(x == 0, both[:rows], both[rows:])

        @pl.when(j > 0)
        def _():
            settle(pick(order, z, j - 1))

        return carry

    lax.fori_loop(0, n, experts, 0)
    settle(pick(order, z, n - 1))

    total = att[...].astype(jnp.float32) + s1[z]
    for away in range(1, n):
        source = (z + away) % n
        remote(zs.at[source], rz.at[source], rz_send.at[source], rz_recv.at[source], {"sp": source}).wait_recv()
        total = total + rz[source].astype(jnp.float32)
    out[...] = total.astype(jnp.bfloat16)

    to_sibling.wait_send()
    to_across.wait_send()
    for b in range(n):
        for d in (1, -1):
            @pl.when(((z - b) * d >= 0) & (z + d >= 0) & (z + d < n))
            def _():
                kv_copy(b, d).wait_send()
                line_copy(b, d).wait_send()

        for copy in spread(b):
            copy.wait_send()
        forward(b).wait_send()
        y_copy(b).wait_send()
        x_copy(b).wait_send()

        @pl.when(b != z)
        def _():
            z_copy(b).wait_send()


def layer_on_device(
    queries_small, keys_small, values_small, queries_large, keys_large, values_large,
    query_gain_small, key_gain_small, query_gain_large, key_gain_large,
    residual_in, out_weight_small, out_weight_large, norm_gain, routes, route_scores,
    expert_gate, expert_up, expert_down,
):
    n = lax.axis_size("sp")
    tokens = queries_small.shape[0]
    rows, width = residual_in.shape
    experts_here, _, hidden = expert_gate.shape
    grid_rows = n * tokens // GRID_W
    small, large = rotary_tables(grid_rows, HS_SMALL), rotary_tables(grid_rows, HS_LARGE)
    row_tab = jnp.asarray(np.stack([small[0][0], small[0][1], large[0][0], large[0][1]]))
    col_tab = jnp.asarray(np.stack([small[1][0], small[1][1], large[1][0], large[1][1]]))
    gains = jnp.stack(
        [
            jnp.tile(query_gain_small, LANES // HS_SMALL),
            jnp.tile(key_gain_small, LANES // HS_SMALL),
            query_gain_large,
            key_gain_large,
        ]
    )
    vmem = pl.BlockSpec(memory_space=pltpu.VMEM)
    anywhere = pl.BlockSpec(memory_space=pl.ANY)
    bf, f32 = jnp.bfloat16, jnp.float32
    dma = pltpu.SemaphoreType.DMA
    scratch = [
        pltpu.VMEM((n, 4, tokens, LANES), bf),
        pltpu.VMEM((3, 2 * tokens, LANES), bf),
        pltpu.VMEM((3, 2 * tokens, LANES), f32),
        pltpu.VMEM((3, 2 * tokens, LANES), f32),
        pltpu.VMEM((3, 2 * tokens, LANES), f32),
        pltpu.VMEM((tokens, 4 * LANES), bf),
        pltpu.VMEM((2 * out_weight_small.shape[0], width), bf),
        pltpu.VMEM(expert_gate.shape, bf),
        pltpu.VMEM(expert_up.shape, bf),
        pltpu.VMEM(expert_down.shape, bf),
        pltpu.VMEM((2 * rows, width), bf),
        pltpu.VMEM((2 * rows, width), bf),
        pltpu.VMEM((rows, width), bf),
        pltpu.VMEM((rows, width), bf),
        pltpu.VMEM((rows, width), bf),
        pltpu.VMEM((n, 2, 2, rows, width + LANES), bf),
        pltpu.VMEM((n, 2 * rows, width), bf),
        pltpu.VMEM((n, 2 * rows, width), bf),
        pltpu.VMEM((n, rows, width), f32),
        pltpu.VMEM((n, rows, width), bf),
        pltpu.VMEM((n, rows, width), bf),
        pltpu.VMEM((n, rows, width), bf),
        pltpu.VMEM((n, rows, width), bf),
        dma((5,)),
        dma((n, 2)), dma((n,)),
        dma((2,)), dma((2,)),
        dma((n, 4)), dma((n,)), dma((n, 2, 2)),
        dma((n,)), dma((n,)),
        dma((n,)), dma((n,)),
        dma((n,)), dma((n,)),
    ]
    return pl.pallas_call(
        functools.partial(layer_kernel, n),
        out_shape=jax.ShapeDtypeStruct((rows, width), bf),
        in_specs=[vmem] * 13 + [anywhere] * 5,
        out_specs=vmem,
        scratch_shapes=scratch,
        compiler_params=pltpu.CompilerParams(
            collective_id=0, has_side_effects=True, vmem_limit_bytes=60 * 1024 * 1024
        ),
    )(
        queries_small, keys_small, values_small, queries_large, keys_large, values_large,
        gains, row_tab, col_tab, residual_in, norm_gain.reshape(1, width), routes, route_scores,
        out_weight_small, out_weight_large, expert_gate, expert_up, expert_down,
    )


def choose(mesh, *arrays):
    sp_count, tp_count = mesh.shape["sp"], mesh.shape["tp"]
    rows, top_count = arrays[14].shape
    experts_here = arrays[16].shape[0]
    expert_count = experts_here * sp_count
    capacity = max(2, (2 * top_count * rows + expert_count - 1) // expert_count)
    tokens = arrays[0].shape[0]
    fits = (
        tp_count == 4
        and expert_count <= LANES // 2
        and tokens == tp_count * rows
        and tokens % GRID_W == 0
        and arrays[1].shape[1] == LANES
        and arrays[4].shape[1] == LANES
        and arrays[0].shape[1] == 2 * LANES
        and arrays[3].shape[1] == 2 * LANES
    )
    if fits and experts_here * capacity >= rows:
        return layer_on_device(*arrays)
    return on_device(*arrays)


def solution(mesh):
    in_specs = (
        P(("grp", "sp"), "tp"),
        P(("grp", "sp"), "tp"),
        P(("grp", "sp"), "tp"),
        P(("grp", "sp"), "tp"),
        P(("grp", "sp"), "tp"),
        P(("grp", "sp"), "tp"),
        P("grp"),
        P("grp"),
        P("grp"),
        P("grp"),
        P(("grp", "sp", "tp"), None),
        P("tp", None),
        P("tp", None),
        P(),
        P(("grp", "sp", "tp"), None),
        P(("grp", "sp", "tp"), None),
        P("sp", None, "tp"),
        P("sp", None, "tp"),
        P("sp", "tp", None),
    )
    out_specs = P(("grp", "sp", "tp"), None)
    return jax.shard_map(
        functools.partial(choose, mesh), mesh=mesh, in_specs=in_specs, out_specs=out_specs, check_vma=False
    )
```

```python
import functools

import jax
import jax.numpy as jnp
import numpy as np
from jax import lax
from jax.experimental import pallas as pl
from jax.experimental.pallas import tpu as pltpu
from jax.sharding import PartitionSpec as P

HS_SMALL = 64
HS_LARGE = 128
GRID_W = 64


theta_base = 10000.0
norm_eps = 1e-06
block_target = 1280


def grid_tables(offset, length, head_size):
    places = offset + jnp.arange(length, dtype=jnp.int32)
    grid_rows = (places // GRID_W).astype(jnp.float32)
    grid_cols = (places % GRID_W).astype(jnp.float32)
    rates = jnp.power(
        theta_base, -2.0 * jnp.arange(head_size // 4, dtype=jnp.float32) / (head_size // 2)
    )
    row_angles = grid_rows[:, None, None] * rates
    col_angles = grid_cols[:, None, None] * rates
    return (jnp.cos(row_angles), jnp.sin(row_angles), jnp.cos(col_angles), jnp.sin(col_angles))


def half_turn(segment, cosine, sine_part):
    half_size = segment.shape[-1] // 2
    leading = segment[..., :half_size]
    trailing = segment[..., half_size:]
    return jnp.concatenate(
        [leading * cosine - trailing * sine_part, trailing * cosine + leading * sine_part], axis=-1
    )


def grid_turn(vectors, tables):
    row_cos, row_sin, col_cos, col_sin = tables
    half_size = vectors.shape[-1] // 2
    return jnp.concatenate(
        [
            half_turn(vectors[..., :half_size], row_cos, row_sin),
            half_turn(vectors[..., half_size:], col_cos, col_sin),
        ],
        axis=-1,
    )


def normed_turn(raw_rows, gain, tables):
    widened = raw_rows.astype(jnp.float32)
    scaled = (
        widened * lax.rsqrt(jnp.mean(widened * widened, axis=-1, keepdims=True) + norm_eps) * gain
    )
    return grid_turn(scaled, tables).astype(jnp.bfloat16)


def block_rows(row_count, shard_rows):
    shards = row_count // shard_rows
    chosen = 1
    for factor in range(1, max(1, block_target // shard_rows) + 1):
        if shards % factor == 0:
            chosen = factor
    return chosen * shard_rows


def attend_block(state, queries, key_rows, value_rows):
    largest, weight_sum, accumulated = state
    head_size = queries.shape[-1]
    kv_local = queries.shape[1]
    key_heads = key_rows.reshape(key_rows.shape[0], kv_local, head_size)
    value_heads = value_rows.reshape(value_rows.shape[0], kv_local, head_size)
    scores = jnp.einsum(
        "qgrd,kgd->qgrk", queries, key_heads, preferred_element_type=jnp.float32
    ) * head_size ** (-0.5)
    peak_score = jnp.maximum(largest, jnp.max(scores, axis=-1))
    shrink = jnp.exp(largest - peak_score)
    weights = jnp.exp(scores - peak_score[..., None])
    weight_sum = weight_sum * shrink + jnp.sum(weights, axis=-1)
    accumulated = accumulated * shrink[..., None] + jnp.einsum(
        "qgrk,kgd->qgrd",
        weights.astype(jnp.bfloat16),
        value_heads,
        preferred_element_type=jnp.float32,
    )
    return (peak_score, weight_sum, accumulated)


def attend_rows(state, queries, key_rows, value_rows):
    row_count = key_rows.shape[0]
    step_rows = block_rows(row_count, queries.shape[0])
    if step_rows == row_count:
        return attend_block(state, queries, key_rows, value_rows)

    def one_block(block_index, carried):
        offset = block_index * step_rows
        return attend_block(
            carried,
            queries,
            lax.dynamic_slice_in_dim(key_rows, offset, step_rows, 0),
            lax.dynamic_slice_in_dim(value_rows, offset, step_rows, 0),
        )

    return lax.fori_loop(0, row_count // step_rows, one_block, state)


def empty_state(queries):
    state_shape = queries.shape[:3]
    return (
        jnp.full(state_shape, -1e30, jnp.float32),
        jnp.zeros(state_shape, jnp.float32),
        jnp.zeros(queries.shape, jnp.float32),
    )


def finish(state):
    largest, weight_sum, accumulated = state
    merged = accumulated / weight_sum[..., None]
    return merged.reshape(merged.shape[0], -1).astype(jnp.bfloat16)


def on_device(
    queries_small,
    keys_small,
    values_small,
    queries_large,
    keys_large,
    values_large,
    query_gain_small,
    key_gain_small,
    query_gain_large,
    key_gain_large,
    residual_in,
    out_weight_small,
    out_weight_large,
    norm_gain,
    routes,
    route_scores,
    expert_gate,
    expert_up,
    expert_down,
):
    token_rows = queries_small.shape[0]
    offset = lax.axis_index("sp") * token_rows
    tables_small = grid_tables(offset, token_rows, HS_SMALL)
    tables_large = grid_tables(offset, token_rows, HS_LARGE)
    kv_small = keys_small.shape[1] // HS_SMALL
    kv_large = keys_large.shape[1] // HS_LARGE
    asked_small = normed_turn(
        queries_small.reshape(token_rows, -1, HS_SMALL), query_gain_small, tables_small
    ).reshape(token_rows, kv_small, -1, HS_SMALL)
    asked_large = normed_turn(
        queries_large.reshape(token_rows, -1, HS_LARGE), query_gain_large, tables_large
    ).reshape(token_rows, kv_large, -1, HS_LARGE)
    turned_small = normed_turn(
        keys_small.reshape(token_rows, kv_small, HS_SMALL), key_gain_small, tables_small
    ).reshape(token_rows, -1)
    turned_large = normed_turn(
        keys_large.reshape(token_rows, kv_large, HS_LARGE), key_gain_large, tables_large
    ).reshape(token_rows, -1)
    key_small = lax.all_gather(turned_small, "sp", axis=0, tiled=True)
    value_small = lax.all_gather(values_small, "sp", axis=0, tiled=True)
    key_large = lax.all_gather(turned_large, "sp", axis=0, tiled=True)
    value_large = lax.all_gather(values_large, "sp", axis=0, tiled=True)
    state_small = attend_rows(empty_state(asked_small), asked_small, key_small, value_small)
    state_large = attend_rows(empty_state(asked_large), asked_large, key_large, value_large)
    heard_small = finish(state_small)
    heard_large = finish(state_large)
    projected = lax.psum_scatter(
        (
            jnp.dot(heard_small, out_weight_small, preferred_element_type=jnp.float32)
            + jnp.dot(heard_large, out_weight_large, preferred_element_type=jnp.float32)
        ).astype(jnp.bfloat16),
        "tp",
        scatter_dimension=0,
        tiled=True,
    ).astype(jnp.float32)
    attended = (residual_in.astype(jnp.float32) + projected).astype(jnp.bfloat16)
    widened = attended.astype(jnp.float32)
    normed = (
        widened
        * lax.rsqrt(jnp.mean(widened * widened, axis=-1, keepdims=True) + norm_eps)
        * norm_gain
    ).astype(jnp.bfloat16)
    local_rows = routes.shape[0]
    top_count = routes.shape[1]
    sp_count = lax.axis_size("sp")
    local_experts = expert_gate.shape[0]
    expert_count = local_experts * sp_count
    capacity = max(2, (2 * top_count * local_rows + expert_count - 1) // expert_count)
    flat_routes = routes.reshape(-1)
    member = (flat_routes[:, None] == jnp.arange(expert_count, dtype=jnp.int32)[None, :]).astype(
        jnp.int32
    )
    ranks = jnp.sum((jnp.cumsum(member, axis=0) - member) * member, axis=1)
    slots = flat_routes * capacity + ranks
    picker = (
        slots[:, None] == jnp.arange(expert_count * capacity, dtype=jnp.int32)[None, :]
    ).astype(jnp.bfloat16)
    placer = jnp.sum(picker.reshape(local_rows, top_count, -1), axis=1)
    outgoing = jnp.einsum("ts,td->sd", placer, normed, preferred_element_type=jnp.float32).astype(
        jnp.bfloat16
    )
    outgoing = outgoing.reshape(sp_count, local_experts, capacity, -1)
    everyone = lax.all_gather(
        lax.all_to_all(outgoing, "sp", split_axis=0, concat_axis=0, tiled=True),
        "tp",
        axis=0,
        tiled=True,
    )
    gate_out = jnp.einsum(
        "secd,edf->secf", everyone, expert_gate, preferred_element_type=jnp.float32
    )
    up_out = jnp.einsum("secd,edf->secf", everyone, expert_up, preferred_element_type=jnp.float32)
    active = (jax.nn.silu(gate_out) * up_out).astype(jnp.bfloat16)
    summed = lax.psum_scatter(
        jnp.einsum(
            "secf,efd->secd", active, expert_down, preferred_element_type=jnp.float32
        ).astype(jnp.bfloat16),
        "tp",
        scatter_dimension=0,
        tiled=True,
    )
    returned = lax.all_to_all(summed, "sp", split_axis=0, concat_axis=0, tiled=True)
    back_rows = returned.reshape(expert_count * capacity, -1)
    chosen_rows = jnp.dot(picker, back_rows, preferred_element_type=jnp.float32).reshape(
        local_rows, top_count, -1
    )
    shares = route_scores / jnp.sum(route_scores, axis=1, keepdims=True)
    mixed = jnp.sum(chosen_rows * shares[:, :, None], axis=1)
    return (attended.astype(jnp.float32) + mixed).astype(jnp.bfloat16)


MESH = pl.DeviceIdType.MESH
LANES = 128


def rotary_tables(grid_rows, head_size):
    lane = np.arange(LANES) % head_size
    rates = np.power(
        np.float32(theta_base),
        (np.float32(-2.0) * np.arange(head_size // 4, dtype=np.float32) / np.float32(head_size // 2)),
    ).astype(np.float32)
    rate = rates[lane % (head_size // 4)]
    is_row = lane < head_size // 2
    sign = np.where(lane % (head_size // 2) < head_size // 4, -1.0, 1.0)

    def build(count, keep):
        angles = np.arange(count, dtype=np.float32)[:, None] * rate[None, :]
        angles = angles.astype(np.float64)
        return (
            np.where(keep, np.cos(angles), 0.0).astype(np.float32),
            np.where(keep, np.sin(angles) * sign, 0.0).astype(np.float32),
        )

    return build(grid_rows, is_row), build(GRID_W, ~is_row)


def visit_order(count):
    return [sorted(range(count), key=lambda b: (abs(b - at), b)) for at in range(count)]


def pick(table, at, step):
    chosen = jnp.int32(0)
    for i, row in enumerate(table):
        for j, entry in enumerate(row):
            chosen = jnp.where((at == i) & (step == j), jnp.int32(entry), chosen)
    return chosen


def lanes_of(shape):
    return lax.broadcasted_iota(jnp.int32, shape, len(shape) - 1)


def turn_rows(raw, gain, cosine, sine, head_size):
    wide = raw.astype(jnp.float32)
    lane = lanes_of(wide.shape)
    squares = wide * wide
    if head_size == LANES:
        scale = lax.rsqrt(jnp.sum(squares, axis=-1, keepdims=True) / head_size + norm_eps)
    else:
        low = lane < head_size
        first = jnp.sum(jnp.where(low, squares, 0.0), axis=-1, keepdims=True) / head_size
        second = jnp.sum(jnp.where(low, 0.0, squares), axis=-1, keepdims=True) / head_size
        scale = jnp.where(low, lax.rsqrt(first + norm_eps), lax.rsqrt(second + norm_eps))
    scaled = wide * scale * gain
    quarter = head_size // 4
    ahead = pltpu.roll(scaled, LANES - quarter, 1)
    behind = pltpu.roll(scaled, quarter, 1)
    partner = jnp.where(lane % (2 * quarter) < quarter, ahead, behind)
    return scaled * cosine + partner * sine


def layer_kernel(
    sp_count,
    q_s, k_s, v_s, q_l, k_l, v_l, gain_qs, gain_ks, gain_ql, gain_kl, row_tab, col_tab, residual, norm_gain, routes, scores,
    ws_any, wl_any, eg_any, eu_any, ed_any,
    out,
    kv, qst, big, den, acc, heard, w_out, w_gate, w_up, w_down,
    p_out, p_in, x_out, x_in, att, ag,
    y_out, y_in, s1, xs, rx, zs, rz,
    w_sem, kv_send, kv_recv, p_send, p_recv, ag_send, ag_fwd, ag_recv,
    yc_send, yc_recv, rx_send, rx_recv, rz_send, rz_recv,
):
    n = sp_count
    z = lax.axis_index("sp")
    tp = lax.axis_index("tp")
    x, c = tp // 2, tp % 2
    sibling = {"tp": x * 2 + (1 - c)}
    across = {"tp": (1 - x) * 2 + c}
    order = visit_order(n)
    tokens = q_s.shape[0]
    rows = residual.shape[0]
    width = residual.shape[1]
    experts_here = eg_any.shape[0]
    hidden = eg_any.shape[2]

    def remote(src, dst, send, recv, to):
        return pltpu.make_async_remote_copy(
            src_ref=src, dst_ref=dst, send_sem=send, recv_sem=recv, device_id=to, device_id_type=MESH
        )

    half = ws_any.shape[0]
    loads = [
        pltpu.make_async_copy(ws_any, w_out.at[pl.ds(0, half)], w_sem.at[0]),
        pltpu.make_async_copy(wl_any, w_out.at[pl.ds(half, half)], w_sem.at[1]),
        pltpu.make_async_copy(eg_any, w_gate, w_sem.at[2]),
        pltpu.make_async_copy(eu_any, w_up, w_sem.at[3]),
        pltpu.make_async_copy(ed_any, w_down, w_sem.at[4]),
    ]
    for load in loads:
        load.start()

    barrier = pltpu.get_barrier_semaphore()
    for away in range(1, n):
        pl.semaphore_signal(barrier, inc=1, device_id={"sp": (z + away) % n}, device_id_type=MESH)
    pl.semaphore_signal(barrier, inc=1, device_id=sibling, device_id_type=MESH)
    pl.semaphore_signal(barrier, inc=1, device_id=across, device_id_type=MESH)

    strips = tokens // GRID_W

    def table(kind):
        pieces = [
            row_tab[kind, pl.ds(z * strips + r, 1), :] + col_tab[kind] for r in range(strips)
        ]
        return jnp.concatenate(pieces, axis=0)

    kv[z, 0, 0] = v_s[...]
    kv[z, 0, 1] = v_l[...]
    cos_s, sin_s, cos_l, sin_l = table(0), table(1), table(2), table(3)

    def kv_copy(b, kind, d):
        block = kv.at[b, kind]
        return remote(
            block, block, kv_send.at[b, kind, (d + 1) // 2], kv_recv.at[b, kind], {"sp": z + d}
        )

    def kv_start(b, kind, ways):
        for d in (1, -1):
            @pl.when(((ways == 0) | (ways == d)) & (z + d >= 0) & (z + d < n))
            def _():
                kv_copy(b, kind, d).start()

    pl.semaphore_wait(barrier, n + 1)
    kv_start(z, 0, 0)

    def both_heads(gain):
        return jnp.concatenate([gain[...]] * (LANES // HS_SMALL), axis=1)

    kv[z, 1, 0] = turn_rows(k_s[...], both_heads(gain_ks), cos_s, sin_s, HS_SMALL).astype(
        jnp.bfloat16
    )
    kv[z, 1, 1] = turn_rows(k_l[...], gain_kl[...], cos_l, sin_l, HS_LARGE).astype(jnp.bfloat16)
    kv_start(z, 1, 0)
    inner = (z > 0) & (z < n - 1)

    low = lanes_of((tokens, LANES)) < HS_SMALL
    zero = jnp.zeros((tokens, LANES), jnp.float32)
    q01 = turn_rows(q_s[:, :LANES], both_heads(gain_qs), cos_s, sin_s, HS_SMALL)
    q23 = turn_rows(q_s[:, LANES:], both_heads(gain_qs), cos_s, sin_s, HS_SMALL)
    qst[0, :tokens] = jnp.where(low, q01, zero).astype(jnp.bfloat16)
    qst[0, tokens:] = jnp.where(low, pltpu.roll(q01, HS_SMALL, 1), zero).astype(jnp.bfloat16)
    qst[1, :tokens] = jnp.where(low, zero, pltpu.roll(q23, HS_SMALL, 1)).astype(jnp.bfloat16)
    qst[1, tokens:] = jnp.where(low, zero, q23).astype(jnp.bfloat16)
    for h in range(2):
        piece = q_l[:, h * LANES : (h + 1) * LANES]
        qst[2, h * tokens : (h + 1) * tokens] = turn_rows(
            piece, gain_ql[...], cos_l, sin_l, HS_LARGE
        ).astype(jnp.bfloat16)
    big[...] = jnp.full(big.shape, -1e30, jnp.float32)
    den[...] = jnp.zeros(den.shape, jnp.float32)
    acc[...] = jnp.zeros(acc.shape, jnp.float32)

    def take(j):
        b = pick(order, z, j)
        d = jnp.where(b < z, 1, -1)
        for kind in range(2):
            kv_copy(b, kind, 1).wait_recv()
            kv_start(b, kind, d)

    def attend(j, carry):
        b = pick(order, z, j)

        @pl.when((j > 0) & ((j != 2) | jnp.logical_not(inner)))
        def _():
            take(j)

        @pl.when((j == 1) & inner)
        def _():
            take(2)

        for g in range(3):
            keys = kv[b, 1, 0 if g < 2 else 1]
            values = kv[b, 0, 0 if g < 2 else 1]
            scale = (HS_SMALL if g < 2 else HS_LARGE) ** (-0.5)
            score = (
                lax.dot_general(
                    qst[g], keys, (((1,), (1,)), ((), ())), preferred_element_type=jnp.float32
                )
                * scale
            )
            before = big[g]
            peak = jnp.maximum(before, jnp.max(score, axis=-1, keepdims=True))
            shrink = jnp.exp(before - peak)
            weight = jnp.exp(score - peak[:, :1])
            den[g] = den[g] * shrink + jnp.sum(weight, axis=-1, keepdims=True)
            acc[g] = acc[g] * shrink + jnp.dot(
                weight.astype(jnp.bfloat16), values, preferred_element_type=jnp.float32
            )
            big[g] = peak
        return carry

    lax.fori_loop(0, n, attend, 0)

    o0, o1, o2 = acc[0] / den[0], acc[1] / den[1], acc[2] / den[2]
    heard[:, 0:LANES] = jnp.where(low, o0[:tokens], pltpu.roll(o0[tokens:], HS_SMALL, 1)).astype(
        jnp.bfloat16
    )
    heard[:, LANES : 2 * LANES] = jnp.where(
        low, pltpu.roll(o1[:tokens], HS_SMALL, 1), o1[tokens:]
    ).astype(jnp.bfloat16)
    heard[:, 2 * LANES : 3 * LANES] = o2[:tokens].astype(jnp.bfloat16)
    heard[:, 3 * LANES : 4 * LANES] = o2[tokens:].astype(jnp.bfloat16)

    loads[0].wait()
    loads[1].wait()

    part = width // 2

    def projected(core, h):
        lhs = jnp.concatenate(
            [heard[pl.ds((xx * 2 + core) * rows, rows), :] for xx in range(2)], axis=0
        )
        return jnp.dot(
            lhs, w_out[:, h * part : (h + 1) * part], preferred_element_type=jnp.float32
        ).astype(jnp.bfloat16)

    def p_copy(h):
        return remote(p_out.at[h], p_in.at[h], p_send.at[0, h], p_recv.at[0, h], sibling)

    def q_copy(h):
        return remote(x_out.at[h], x_in.at[h], p_send.at[1, h], p_recv.at[1, h], across)

    for h in range(2):
        p_out[h] = projected(1 - c, h)
        p_copy(h).start()
    here_first = x == 0
    for h in range(2):
        own_term = projected(c, h).astype(jnp.float32)
        p_copy(h).wait_recv()
        pair = own_term + p_in[h].astype(jnp.float32)
        x_out[h] = jnp.where(here_first, pair[rows:], pair[:rows]).astype(jnp.bfloat16)
        q_copy(h).start()
        cols = slice(h * part, (h + 1) * part)
        s1[0, :, cols] = jnp.where(here_first, pair[:rows], pair[rows:]) + residual[
            :, cols
        ].astype(jnp.float32)

    share = scores[...] / jnp.sum(scores[...], axis=0, keepdims=True)
    names = lax.broadcasted_iota(jnp.int32, (LANES // 2, rows), 0)
    dense = jnp.zeros((LANES // 2, rows), jnp.float32)
    for t in range(routes.shape[0]):
        dense = jnp.where(names == routes[t : t + 1, :], share[t : t + 1, :], dense)
    dense_high = dense.astype(jnp.bfloat16).astype(jnp.float32)
    packed = jnp.concatenate([dense_high, dense - dense_high], axis=0)
    ag[z, x, c, :, width:] = jnp.transpose(packed).astype(jnp.bfloat16)

    for h in range(2):
        cols = slice(h * part, (h + 1) * part)
        q_copy(h).wait_recv()
        att[:, cols] = (s1[0, :, cols] + x_in[h].astype(jnp.float32)).astype(jnp.bfloat16)
    attended = att[...]
    wide = attended.astype(jnp.float32)
    ag[z, x, c, :, :width] = (
        wide
        * lax.rsqrt(jnp.sum(wide * wide, axis=-1, keepdims=True) / width + norm_eps)
        * norm_gain[...]
    ).astype(jnp.bfloat16)

    def ag_copy(b, xx, cc, sem, to):
        block = ag.at[b, xx, cc]
        return remote(block, block, sem, ag_recv.at[b, xx, cc], to)

    def line_copy(b, d):
        return ag_copy(b, x, c, ag_send.at[b, (d + 1) // 2], {"sp": z + d})

    def spread(b):
        return (
            ag_copy(b, x, c, ag_send.at[b, 2], across),
            ag_copy(b, x, c, ag_send.at[b, 3], sibling),
        )

    def forward(b):
        return ag_copy(b, 1 - x, c, ag_fwd.at[b], sibling)

    for d in (1, -1):
        @pl.when((z + d >= 0) & (z + d < n))
        def _():
            line_copy(z, d).start()

    for copy in spread(z):
        copy.start()

    def y_copy(b):
        return remote(y_out.at[b], y_in.at[b], yc_send.at[b], yc_recv.at[b], sibling)

    def x_copy(b):
        return remote(xs.at[b], rx.at[b], rx_send.at[b], rx_recv.at[b], across)

    def z_copy(b):
        return remote(zs.at[b], rz.at[z], rz_send.at[b], rz_recv.at[z], {"sp": b})

    def settle(b):
        x_copy(b).wait_recv()
        total = s1[b] + rx[b].astype(jnp.float32)

        @pl.when(b == z)
        def _():
            s1[b] = total

        @pl.when(b != z)
        def _():
            zs[b] = total.astype(jnp.bfloat16)
            z_copy(b).start()

    for load in loads[2:]:
        load.wait()

    def experts(j, carry):
        b = pick(order, z, j)

        def gain_block(step):
            later = pick(order, z, step)
            ag_copy(later, x, c, ag_send.at[later, 2], across).wait_recv()
            for way in (1, -1):
                @pl.when((jnp.where(later < z, 1, -1) == way) & (z + way >= 0) & (z + way < n))
                def _():
                    line_copy(later, way).start()

            for copy in spread(later):
                copy.start()

        ahead = j + jnp.where(inner & (j > 0), 2, 1)

        @pl.when(ahead < n)
        def _():
            gain_block(ahead)

        @pl.when(inner & (j == 0))
        def _():
            gain_block(2)

        ag_copy(b, 1 - x, c, ag_fwd.at[b], sibling).wait_recv()
        forward(b).start()
        for xx in (x, 1 - x):
            ag_copy(b, xx, 1 - c, ag_fwd.at[b], sibling).wait_recv()
        blocks = [ag[b, xx, cc] for cc in (1 - c, c) for xx in range(2)]
        rows_in = jnp.concatenate([block[:, :width] for block in blocks], axis=0)
        marks = jnp.concatenate([block[:, width:] for block in blocks], axis=0).astype(jnp.float32)
        mark_lane = lanes_of(marks.shape) % (LANES // 2)
        active = []
        for e in range(experts_here):
            gate = jnp.dot(rows_in, w_gate[e], preferred_element_type=jnp.float32)
            up = jnp.dot(rows_in, w_up[e], preferred_element_type=jnp.float32)
            weight = jnp.sum(
                jnp.where(mark_lane == z * experts_here + e, marks, 0.0), axis=1, keepdims=True
            )
            active.append((gate / (1.0 + jnp.exp(-gate)) * up * weight).astype(jnp.bfloat16))
        hidden_rows = jnp.concatenate(active, axis=1)
        down = w_down[...].reshape(experts_here * hidden, width)
        split = 2 * rows
        y_out[b] = jnp.dot(
            hidden_rows[:split], down, preferred_element_type=jnp.float32
        ).astype(jnp.bfloat16)
        y_copy(b).start()
        mine = jnp.dot(hidden_rows[split:], down, preferred_element_type=jnp.float32)
        y_copy(b).wait_recv()
        both = mine + y_in[b].astype(jnp.float32)
        xs[b] = jnp.where(x == 0, both[rows:], both[:rows]).astype(jnp.bfloat16)
        x_copy(b).start()
        s1[b] = jnp.where(x == 0, both[:rows], both[rows:])

        @pl.when(j > 1)
        def _():
            settle(pick(order, z, j - 2))

        return carry

    lax.fori_loop(0, n, experts, 0)
    settle(pick(order, z, n - 2))
    settle(pick(order, z, n - 1))

    total = att[...].astype(jnp.float32) + s1[z]
    for away in range(1, n):
        source = (z + away) % n
        remote(zs.at[source], rz.at[source], rz_send.at[source], rz_recv.at[source], {"sp": source}).wait_recv()
        total = total + rz[source].astype(jnp.float32)
    out[...] = total.astype(jnp.bfloat16)

    for h in range(2):
        p_copy(h).wait_send()
        q_copy(h).wait_send()
    for b in range(n):
        for d in (1, -1):
            @pl.when(((z - b) * d >= 0) & (z + d >= 0) & (z + d < n))
            def _():
                for kind in range(2):
                    kv_copy(b, kind, d).wait_send()
                line_copy(b, d).wait_send()

        for copy in spread(b):
            copy.wait_send()
        forward(b).wait_send()
        y_copy(b).wait_send()
        x_copy(b).wait_send()

        @pl.when(b != z)
        def _():
            z_copy(b).wait_send()


def layer_on_device(
    queries_small, keys_small, values_small, queries_large, keys_large, values_large,
    query_gain_small, key_gain_small, query_gain_large, key_gain_large,
    residual_in, out_weight_small, out_weight_large, norm_gain, routes, route_scores,
    expert_gate, expert_up, expert_down,
):
    n = lax.axis_size("sp")
    tokens = queries_small.shape[0]
    rows, width = residual_in.shape
    experts_here, _, hidden = expert_gate.shape
    grid_rows = n * tokens // GRID_W
    small, large = rotary_tables(grid_rows, HS_SMALL), rotary_tables(grid_rows, HS_LARGE)
    row_tab = jnp.asarray(np.stack([small[0][0], small[0][1], large[0][0], large[0][1]]))
    col_tab = jnp.asarray(np.stack([small[1][0], small[1][1], large[1][0], large[1][1]]))
    gains = [
        gain.reshape(1, -1)
        for gain in (query_gain_small, key_gain_small, query_gain_large, key_gain_large)
    ]
    vmem = pl.BlockSpec(memory_space=pltpu.VMEM)
    anywhere = pl.BlockSpec(memory_space=pl.ANY)
    bf, f32 = jnp.bfloat16, jnp.float32
    dma = pltpu.SemaphoreType.DMA
    scratch = [
        pltpu.VMEM((n, 2, 2, tokens, LANES), bf),
        pltpu.VMEM((3, 2 * tokens, LANES), bf),
        pltpu.VMEM((3, 2 * tokens, LANES), f32),
        pltpu.VMEM((3, 2 * tokens, LANES), f32),
        pltpu.VMEM((3, 2 * tokens, LANES), f32),
        pltpu.VMEM((tokens, 4 * LANES), bf),
        pltpu.VMEM((2 * out_weight_small.shape[0], width), bf),
        pltpu.VMEM(expert_gate.shape, bf),
        pltpu.VMEM(expert_up.shape, bf),
        pltpu.VMEM(expert_down.shape, bf),
        pltpu.VMEM((2, 2 * rows, width // 2), bf),
        pltpu.VMEM((2, 2 * rows, width // 2), bf),
        pltpu.VMEM((2, rows, width // 2), bf),
        pltpu.VMEM((2, rows, width // 2), bf),
        pltpu.VMEM((rows, width), bf),
        pltpu.VMEM((n, 2, 2, rows, width + LANES), bf),
        pltpu.VMEM((n, 2 * rows, width), bf),
        pltpu.VMEM((n, 2 * rows, width), bf),
        pltpu.VMEM((n, rows, width), f32),
        pltpu.VMEM((n, rows, width), bf),
        pltpu.VMEM((n, rows, width), bf),
        pltpu.VMEM((n, rows, width), bf),
        pltpu.VMEM((n, rows, width), bf),
        dma((5,)),
        dma((n, 2, 2)), dma((n, 2)),
        dma((2, 2)), dma((2, 2)),
        dma((n, 4)), dma((n,)), dma((n, 2, 2)),
        dma((n,)), dma((n,)),
        dma((n,)), dma((n,)),
        dma((n,)), dma((n,)),
    ]
    return pl.pallas_call(
        functools.partial(layer_kernel, n),
        out_shape=jax.ShapeDtypeStruct((rows, width), bf),
        in_specs=[vmem] * 16 + [anywhere] * 5,
        out_specs=vmem,
        scratch_shapes=scratch,
        compiler_params=pltpu.CompilerParams(
            collective_id=0, has_side_effects=True, vmem_limit_bytes=60 * 1024 * 1024
        ),
    )(
        queries_small, keys_small, values_small, queries_large, keys_large, values_large,
        *gains, row_tab, col_tab, residual_in, norm_gain.reshape(1, width), routes.T, route_scores.T,
        out_weight_small, out_weight_large, expert_gate, expert_up, expert_down,
    )


def choose(mesh, *arrays):
    sp_count, tp_count = mesh.shape["sp"], mesh.shape["tp"]
    rows, top_count = arrays[14].shape
    experts_here = arrays[16].shape[0]
    expert_count = experts_here * sp_count
    capacity = max(2, (2 * top_count * rows + expert_count - 1) // expert_count)
    tokens = arrays[0].shape[0]
    fits = (
        tp_count == 4
        and sp_count > 1
        and expert_count <= LANES // 2
        and tokens == tp_count * rows
        and tokens % GRID_W == 0
        and arrays[1].shape[1] == LANES
        and arrays[4].shape[1] == LANES
        and arrays[0].shape[1] == 2 * LANES
        and arrays[3].shape[1] == 2 * LANES
    )
    if fits and experts_here * capacity >= rows:
        return layer_on_device(*arrays)
    return on_device(*arrays)


def solution(mesh):
    in_specs = (
        P(("grp", "sp"), "tp"),
        P(("grp", "sp"), "tp"),
        P(("grp", "sp"), "tp"),
        P(("grp", "sp"), "tp"),
        P(("grp", "sp"), "tp"),
        P(("grp", "sp"), "tp"),
        P("grp"),
        P("grp"),
        P("grp"),
        P("grp"),
        P(("grp", "sp", "tp"), None),
        P("tp", None),
        P("tp", None),
        P(),
        P(("grp", "sp", "tp"), None),
        P(("grp", "sp", "tp"), None),
        P("sp", None, "tp"),
        P("sp", None, "tp"),
        P("sp", "tp", None),
    )
    out_specs = P(("grp", "sp", "tp"), None)
    return jax.shard_map(
        functools.partial(choose, mesh), mesh=mesh, in_specs=in_specs, out_specs=out_specs, check_vma=False
    )
```

```python
import functools

import jax
import jax.numpy as jnp
import numpy as np
from jax import lax
from jax.experimental import pallas as pl
from jax.experimental.pallas import tpu as pltpu
from jax.sharding import PartitionSpec as P

HS_SMALL = 64
HS_LARGE = 128
GRID_W = 64


theta_base = 10000.0
norm_eps = 1e-06
block_target = 1280


def grid_tables(offset, length, head_size):
    places = offset + jnp.arange(length, dtype=jnp.int32)
    grid_rows = (places // GRID_W).astype(jnp.float32)
    grid_cols = (places % GRID_W).astype(jnp.float32)
    rates = jnp.power(
        theta_base, -2.0 * jnp.arange(head_size // 4, dtype=jnp.float32) / (head_size // 2)
    )
    row_angles = grid_rows[:, None, None] * rates
    col_angles = grid_cols[:, None, None] * rates
    return (jnp.cos(row_angles), jnp.sin(row_angles), jnp.cos(col_angles), jnp.sin(col_angles))


def half_turn(segment, cosine, sine_part):
    half_size = segment.shape[-1] // 2
    leading = segment[..., :half_size]
    trailing = segment[..., half_size:]
    return jnp.concatenate(
        [leading * cosine - trailing * sine_part, trailing * cosine + leading * sine_part], axis=-1
    )


def grid_turn(vectors, tables):
    row_cos, row_sin, col_cos, col_sin = tables
    half_size = vectors.shape[-1] // 2
    return jnp.concatenate(
        [
            half_turn(vectors[..., :half_size], row_cos, row_sin),
            half_turn(vectors[..., half_size:], col_cos, col_sin),
        ],
        axis=-1,
    )


def normed_turn(raw_rows, gain, tables):
    widened = raw_rows.astype(jnp.float32)
    scaled = (
        widened * lax.rsqrt(jnp.mean(widened * widened, axis=-1, keepdims=True) + norm_eps) * gain
    )
    return grid_turn(scaled, tables).astype(jnp.bfloat16)


def block_rows(row_count, shard_rows):
    shards = row_count // shard_rows
    chosen = 1
    for factor in range(1, max(1, block_target // shard_rows) + 1):
        if shards % factor == 0:
            chosen = factor
    return chosen * shard_rows


def attend_block(state, queries, key_rows, value_rows):
    largest, weight_sum, accumulated = state
    head_size = queries.shape[-1]
    kv_local = queries.shape[1]
    key_heads = key_rows.reshape(key_rows.shape[0], kv_local, head_size)
    value_heads = value_rows.reshape(value_rows.shape[0], kv_local, head_size)
    scores = jnp.einsum(
        "qgrd,kgd->qgrk", queries, key_heads, preferred_element_type=jnp.float32
    ) * head_size ** (-0.5)
    peak_score = jnp.maximum(largest, jnp.max(scores, axis=-1))
    shrink = jnp.exp(largest - peak_score)
    weights = jnp.exp(scores - peak_score[..., None])
    weight_sum = weight_sum * shrink + jnp.sum(weights, axis=-1)
    accumulated = accumulated * shrink[..., None] + jnp.einsum(
        "qgrk,kgd->qgrd",
        weights.astype(jnp.bfloat16),
        value_heads,
        preferred_element_type=jnp.float32,
    )
    return (peak_score, weight_sum, accumulated)


def attend_rows(state, queries, key_rows, value_rows):
    row_count = key_rows.shape[0]
    step_rows = block_rows(row_count, queries.shape[0])
    if step_rows == row_count:
        return attend_block(state, queries, key_rows, value_rows)

    def one_block(block_index, carried):
        offset = block_index * step_rows
        return attend_block(
            carried,
            queries,
            lax.dynamic_slice_in_dim(key_rows, offset, step_rows, 0),
            lax.dynamic_slice_in_dim(value_rows, offset, step_rows, 0),
        )

    return lax.fori_loop(0, row_count // step_rows, one_block, state)


def empty_state(queries):
    state_shape = queries.shape[:3]
    return (
        jnp.full(state_shape, -1e30, jnp.float32),
        jnp.zeros(state_shape, jnp.float32),
        jnp.zeros(queries.shape, jnp.float32),
    )


def finish(state):
    largest, weight_sum, accumulated = state
    merged = accumulated / weight_sum[..., None]
    return merged.reshape(merged.shape[0], -1).astype(jnp.bfloat16)


def on_device(
    queries_small,
    keys_small,
    values_small,
    queries_large,
    keys_large,
    values_large,
    query_gain_small,
    key_gain_small,
    query_gain_large,
    key_gain_large,
    residual_in,
    out_weight_small,
    out_weight_large,
    norm_gain,
    routes,
    route_scores,
    expert_gate,
    expert_up,
    expert_down,
):
    token_rows = queries_small.shape[0]
    offset = lax.axis_index("sp") * token_rows
    tables_small = grid_tables(offset, token_rows, HS_SMALL)
    tables_large = grid_tables(offset, token_rows, HS_LARGE)
    kv_small = keys_small.shape[1] // HS_SMALL
    kv_large = keys_large.shape[1] // HS_LARGE
    asked_small = normed_turn(
        queries_small.reshape(token_rows, -1, HS_SMALL), query_gain_small, tables_small
    ).reshape(token_rows, kv_small, -1, HS_SMALL)
    asked_large = normed_turn(
        queries_large.reshape(token_rows, -1, HS_LARGE), query_gain_large, tables_large
    ).reshape(token_rows, kv_large, -1, HS_LARGE)
    turned_small = normed_turn(
        keys_small.reshape(token_rows, kv_small, HS_SMALL), key_gain_small, tables_small
    ).reshape(token_rows, -1)
    turned_large = normed_turn(
        keys_large.reshape(token_rows, kv_large, HS_LARGE), key_gain_large, tables_large
    ).reshape(token_rows, -1)
    key_small = lax.all_gather(turned_small, "sp", axis=0, tiled=True)
    value_small = lax.all_gather(values_small, "sp", axis=0, tiled=True)
    key_large = lax.all_gather(turned_large, "sp", axis=0, tiled=True)
    value_large = lax.all_gather(values_large, "sp", axis=0, tiled=True)
    state_small = attend_rows(empty_state(asked_small), asked_small, key_small, value_small)
    state_large = attend_rows(empty_state(asked_large), asked_large, key_large, value_large)
    heard_small = finish(state_small)
    heard_large = finish(state_large)
    projected = lax.psum_scatter(
        (
            jnp.dot(heard_small, out_weight_small, preferred_element_type=jnp.float32)
            + jnp.dot(heard_large, out_weight_large, preferred_element_type=jnp.float32)
        ).astype(jnp.bfloat16),
        "tp",
        scatter_dimension=0,
        tiled=True,
    ).astype(jnp.float32)
    attended = (residual_in.astype(jnp.float32) + projected).astype(jnp.bfloat16)
    widened = attended.astype(jnp.float32)
    normed = (
        widened
        * lax.rsqrt(jnp.mean(widened * widened, axis=-1, keepdims=True) + norm_eps)
        * norm_gain
    ).astype(jnp.bfloat16)
    local_rows = routes.shape[0]
    top_count = routes.shape[1]
    sp_count = lax.axis_size("sp")
    local_experts = expert_gate.shape[0]
    expert_count = local_experts * sp_count
    capacity = max(2, (2 * top_count * local_rows + expert_count - 1) // expert_count)
    flat_routes = routes.reshape(-1)
    member = (flat_routes[:, None] == jnp.arange(expert_count, dtype=jnp.int32)[None, :]).astype(
        jnp.int32
    )
    ranks = jnp.sum((jnp.cumsum(member, axis=0) - member) * member, axis=1)
    slots = flat_routes * capacity + ranks
    picker = (
        slots[:, None] == jnp.arange(expert_count * capacity, dtype=jnp.int32)[None, :]
    ).astype(jnp.bfloat16)
    placer = jnp.sum(picker.reshape(local_rows, top_count, -1), axis=1)
    outgoing = jnp.einsum("ts,td->sd", placer, normed, preferred_element_type=jnp.float32).astype(
        jnp.bfloat16
    )
    outgoing = outgoing.reshape(sp_count, local_experts, capacity, -1)
    everyone = lax.all_gather(
        lax.all_to_all(outgoing, "sp", split_axis=0, concat_axis=0, tiled=True),
        "tp",
        axis=0,
        tiled=True,
    )
    gate_out = jnp.einsum(
        "secd,edf->secf", everyone, expert_gate, preferred_element_type=jnp.float32
    )
    up_out = jnp.einsum("secd,edf->secf", everyone, expert_up, preferred_element_type=jnp.float32)
    active = (jax.nn.silu(gate_out) * up_out).astype(jnp.bfloat16)
    summed = lax.psum_scatter(
        jnp.einsum(
            "secf,efd->secd", active, expert_down, preferred_element_type=jnp.float32
        ).astype(jnp.bfloat16),
        "tp",
        scatter_dimension=0,
        tiled=True,
    )
    returned = lax.all_to_all(summed, "sp", split_axis=0, concat_axis=0, tiled=True)
    back_rows = returned.reshape(expert_count * capacity, -1)
    chosen_rows = jnp.dot(picker, back_rows, preferred_element_type=jnp.float32).reshape(
        local_rows, top_count, -1
    )
    shares = route_scores / jnp.sum(route_scores, axis=1, keepdims=True)
    mixed = jnp.sum(chosen_rows * shares[:, :, None], axis=1)
    return (attended.astype(jnp.float32) + mixed).astype(jnp.bfloat16)


MESH = pl.DeviceIdType.MESH
LANES = 128


def rotary_tables(grid_rows, head_size):
    lane = np.arange(LANES) % head_size
    rates = np.power(
        np.float32(theta_base),
        (np.float32(-2.0) * np.arange(head_size // 4, dtype=np.float32) / np.float32(head_size // 2)),
    ).astype(np.float32)
    rate = rates[lane % (head_size // 4)]
    is_row = lane < head_size // 2
    sign = np.where(lane % (head_size // 2) < head_size // 4, -1.0, 1.0)

    def build(count, keep):
        angles = np.arange(count, dtype=np.float32)[:, None] * rate[None, :]
        angles = angles.astype(np.float64)
        return (
            np.where(keep, np.cos(angles), 0.0).astype(np.float32),
            np.where(keep, np.sin(angles) * sign, 0.0).astype(np.float32),
        )

    return build(grid_rows, is_row), build(GRID_W, ~is_row)


def visit_order(count):
    return [sorted(range(count), key=lambda b: (abs(b - at), b)) for at in range(count)]


def pick(table, at, step):
    chosen = jnp.int32(0)
    for i, row in enumerate(table):
        for j, entry in enumerate(row):
            chosen = jnp.where((at == i) & (step == j), jnp.int32(entry), chosen)
    return chosen


def lanes_of(shape):
    return lax.broadcasted_iota(jnp.int32, shape, len(shape) - 1)


def turn_rows(raw, gain, cosine, sine, head_size):
    wide = raw.astype(jnp.float32)
    lane = lanes_of(wide.shape)
    squares = wide * wide
    if head_size == LANES:
        scale = lax.rsqrt(jnp.sum(squares, axis=-1, keepdims=True) / head_size + norm_eps)
    else:
        low = lane < head_size
        first = jnp.sum(jnp.where(low, squares, 0.0), axis=-1, keepdims=True) / head_size
        second = jnp.sum(jnp.where(low, 0.0, squares), axis=-1, keepdims=True) / head_size
        scale = jnp.where(low, lax.rsqrt(first + norm_eps), lax.rsqrt(second + norm_eps))
    scaled = wide * scale * gain
    quarter = head_size // 4
    ahead = pltpu.roll(scaled, LANES - quarter, 1)
    behind = pltpu.roll(scaled, quarter, 1)
    partner = jnp.where(lane % (2 * quarter) < quarter, ahead, behind)
    return scaled * cosine + partner * sine


def layer_kernel(
    sp_count,
    q_s, k_s, v_s, q_l, k_l, v_l, gain_qs, gain_ks, gain_ql, gain_kl, row_tab, col_tab, residual, norm_gain, routes, scores,
    ws_any, wl_any, eg_any, eu_any, ed_any,
    out,
    kv, qst, big, den, acc, heard, w_out, w_gate, w_up, w_down,
    p_out, p_in, x_out, x_in, att, ag,
    y_out, y_in, s1, xs, rx, zs, rz,
    w_sem, kv_send, kv_recv, p_send, p_recv, ag_send, ag_fwd, ag_recv,
    yc_send, yc_recv, rx_send, rx_recv, rz_send, rz_recv,
):
    n = sp_count
    z = lax.axis_index("sp")
    tp = lax.axis_index("tp")
    x, c = tp // 2, tp % 2
    sibling = {"tp": x * 2 + (1 - c)}
    across = {"tp": (1 - x) * 2 + c}
    order = visit_order(n)
    tokens = q_s.shape[0]
    rows = residual.shape[0]
    width = residual.shape[1]
    experts_here = eg_any.shape[0]
    hidden = eg_any.shape[2]

    def remote(src, dst, send, recv, to):
        return pltpu.make_async_remote_copy(
            src_ref=src, dst_ref=dst, send_sem=send, recv_sem=recv, device_id=to, device_id_type=MESH
        )

    half = ws_any.shape[0]
    loads = [
        pltpu.make_async_copy(ws_any, w_out.at[pl.ds(0, half)], w_sem.at[0]),
        pltpu.make_async_copy(wl_any, w_out.at[pl.ds(half, half)], w_sem.at[1]),
        pltpu.make_async_copy(eg_any, w_gate, w_sem.at[2]),
        pltpu.make_async_copy(eu_any, w_up, w_sem.at[3]),
        pltpu.make_async_copy(ed_any, w_down, w_sem.at[4]),
    ]
    for load in loads:
        load.start()

    barrier = pltpu.get_barrier_semaphore()
    for away in range(1, n):
        pl.semaphore_signal(barrier, inc=1, device_id={"sp": (z + away) % n}, device_id_type=MESH)
    pl.semaphore_signal(barrier, inc=1, device_id=sibling, device_id_type=MESH)
    pl.semaphore_signal(barrier, inc=1, device_id=across, device_id_type=MESH)

    strips = tokens // GRID_W

    def table(kind):
        pieces = [
            row_tab[kind, pl.ds(z * strips + r, 1), :] + col_tab[kind] for r in range(strips)
        ]
        return jnp.concatenate(pieces, axis=0)

    kv[z, 0, 0] = v_s[...]
    kv[z, 0, 1] = v_l[...]
    cos_s, sin_s, cos_l, sin_l = table(0), table(1), table(2), table(3)

    def kv_copy(b, kind, d):
        block = kv.at[b, kind]
        return remote(
            block, block, kv_send.at[b, kind, (d + 1) // 2], kv_recv.at[b, kind], {"sp": z + d}
        )

    def kv_start(b, kind, ways):
        for d in (1, -1):
            @pl.when(((ways == 0) | (ways == d)) & (z + d >= 0) & (z + d < n))
            def _():
                kv_copy(b, kind, d).start()

    pl.semaphore_wait(barrier, n + 1)
    kv_start(z, 0, 0)

    def both_heads(gain):
        return jnp.concatenate([gain[...]] * (LANES // HS_SMALL), axis=1)

    kv[z, 1, 0] = turn_rows(k_s[...], both_heads(gain_ks), cos_s, sin_s, HS_SMALL).astype(
        jnp.bfloat16
    )
    kv[z, 1, 1] = turn_rows(k_l[...], gain_kl[...], cos_l, sin_l, HS_LARGE).astype(jnp.bfloat16)
    kv_start(z, 1, 0)
    inner = (z > 0) & (z < n - 1)

    low = lanes_of((tokens, LANES)) < HS_SMALL
    zero = jnp.zeros((tokens, LANES), jnp.float32)
    q01 = turn_rows(q_s[:, :LANES], both_heads(gain_qs), cos_s, sin_s, HS_SMALL)
    q23 = turn_rows(q_s[:, LANES:], both_heads(gain_qs), cos_s, sin_s, HS_SMALL)
    qst[0, :tokens] = jnp.where(low, q01, zero).astype(jnp.bfloat16)
    qst[0, tokens:] = jnp.where(low, pltpu.roll(q01, HS_SMALL, 1), zero).astype(jnp.bfloat16)
    qst[1, :tokens] = jnp.where(low, zero, pltpu.roll(q23, HS_SMALL, 1)).astype(jnp.bfloat16)
    qst[1, tokens:] = jnp.where(low, zero, q23).astype(jnp.bfloat16)
    for h in range(2):
        piece = q_l[:, h * LANES : (h + 1) * LANES]
        qst[2, h * tokens : (h + 1) * tokens] = turn_rows(
            piece, gain_ql[...], cos_l, sin_l, HS_LARGE
        ).astype(jnp.bfloat16)
    big[...] = jnp.full(big.shape, -1e30, jnp.float32)
    den[...] = jnp.zeros(den.shape, jnp.float32)
    acc[...] = jnp.zeros(acc.shape, jnp.float32)

    def take(j):
        b = pick(order, z, j)
        d = jnp.where(b < z, 1, -1)
        for kind in range(2):
            kv_copy(b, kind, 1).wait_recv()
            kv_start(b, kind, d)

    def attend(j, carry):
        b = pick(order, z, j)

        @pl.when((j > 0) & ((j != 2) | jnp.logical_not(inner)))
        def _():
            take(j)

        @pl.when((j == 1) & inner)
        def _():
            take(2)

        for g in range(3):
            keys = kv[b, 1, 0 if g < 2 else 1]
            values = kv[b, 0, 0 if g < 2 else 1]
            scale = (HS_SMALL if g < 2 else HS_LARGE) ** (-0.5)
            score = (
                lax.dot_general(
                    qst[g], keys, (((1,), (1,)), ((), ())), preferred_element_type=jnp.float32
                )
                * scale
            )
            before = big[g]
            peak = jnp.maximum(before, jnp.max(score, axis=-1, keepdims=True))
            shrink = jnp.exp(before - peak)
            weight = jnp.exp(score - peak[:, :1])
            den[g] = den[g] * shrink + jnp.sum(weight, axis=-1, keepdims=True)
            acc[g] = acc[g] * shrink + jnp.dot(
                weight.astype(jnp.bfloat16), values, preferred_element_type=jnp.float32
            )
            big[g] = peak
        return carry

    lax.fori_loop(0, n, attend, 0)

    o0, o1, o2 = acc[0] / den[0], acc[1] / den[1], acc[2] / den[2]
    heard[:, 0:LANES] = jnp.where(low, o0[:tokens], pltpu.roll(o0[tokens:], HS_SMALL, 1)).astype(
        jnp.bfloat16
    )
    heard[:, LANES : 2 * LANES] = jnp.where(
        low, pltpu.roll(o1[:tokens], HS_SMALL, 1), o1[tokens:]
    ).astype(jnp.bfloat16)
    heard[:, 2 * LANES : 3 * LANES] = o2[:tokens].astype(jnp.bfloat16)
    heard[:, 3 * LANES : 4 * LANES] = o2[tokens:].astype(jnp.bfloat16)

    loads[0].wait()
    loads[1].wait()

    part = width // 2

    def projected(core, h):
        lhs = jnp.concatenate(
            [heard[pl.ds((xx * 2 + core) * rows, rows), :] for xx in range(2)], axis=0
        )
        return jnp.dot(
            lhs, w_out[:, h * part : (h + 1) * part], preferred_element_type=jnp.float32
        ).astype(jnp.bfloat16)

    def p_copy(h):
        return remote(p_out.at[h], p_in.at[h], p_send.at[0, h], p_recv.at[0, h], sibling)

    def q_copy(h):
        return remote(x_out.at[h], x_in.at[h], p_send.at[1, h], p_recv.at[1, h], across)

    for h in range(2):
        p_out[h] = projected(1 - c, h)
        p_copy(h).start()
    here_first = x == 0
    for h in range(2):
        own_term = projected(c, h).astype(jnp.float32)
        p_copy(h).wait_recv()
        pair = own_term + p_in[h].astype(jnp.float32)
        x_out[h] = jnp.where(here_first, pair[rows:], pair[:rows]).astype(jnp.bfloat16)
        q_copy(h).start()
        cols = slice(h * part, (h + 1) * part)
        s1[0, :, cols] = jnp.where(here_first, pair[:rows], pair[rows:]) + residual[
            :, cols
        ].astype(jnp.float32)

    share = scores[...] / jnp.sum(scores[...], axis=0, keepdims=True)
    names = lax.broadcasted_iota(jnp.int32, (LANES // 2, rows), 0)
    dense = jnp.zeros((LANES // 2, rows), jnp.float32)
    for t in range(routes.shape[0]):
        dense = jnp.where(names == routes[t : t + 1, :], share[t : t + 1, :], dense)
    dense_high = dense.astype(jnp.bfloat16).astype(jnp.float32)
    packed = jnp.concatenate([dense_high, dense - dense_high], axis=0)
    ag[z, x, c, :, width:] = jnp.transpose(packed).astype(jnp.bfloat16)

    for h in range(2):
        cols = slice(h * part, (h + 1) * part)
        q_copy(h).wait_recv()
        att[:, cols] = (s1[0, :, cols] + x_in[h].astype(jnp.float32)).astype(jnp.bfloat16)
    attended = att[...]
    wide = attended.astype(jnp.float32)
    ag[z, x, c, :, :width] = (
        wide
        * lax.rsqrt(jnp.sum(wide * wide, axis=-1, keepdims=True) / width + norm_eps)
        * norm_gain[...]
    ).astype(jnp.bfloat16)

    def ag_copy(b, xx, cc, sem, to):
        block = ag.at[b, xx, cc]
        return remote(block, block, sem, ag_recv.at[b, xx, cc], to)

    def line_copy(b, d):
        return ag_copy(b, x, c, ag_send.at[b, (d + 1) // 2], {"sp": z + d})

    def spread(b):
        return (
            ag_copy(b, x, c, ag_send.at[b, 2], across),
            ag_copy(b, x, c, ag_send.at[b, 3], sibling),
        )

    def forward(b):
        return ag_copy(b, 1 - x, c, ag_fwd.at[b], sibling)

    for d in (1, -1):
        @pl.when((z + d >= 0) & (z + d < n))
        def _():
            line_copy(z, d).start()

    for copy in spread(z):
        copy.start()

    def y_copy(b):
        return remote(y_out.at[b], y_in.at[b], yc_send.at[b], yc_recv.at[b], sibling)

    def x_copy(b):
        return remote(xs.at[b], rx.at[b], rx_send.at[b], rx_recv.at[b], across)

    def z_copy(b):
        return remote(zs.at[b], rz.at[z], rz_send.at[b], rz_recv.at[z], {"sp": b})

    def settle(b):
        x_copy(b).wait_recv()
        total = s1[b] + rx[b].astype(jnp.float32)

        @pl.when(b == z)
        def _():
            s1[b] = total

        @pl.when(b != z)
        def _():
            zs[b] = total.astype(jnp.bfloat16)
            z_copy(b).start()

    for load in loads[2:]:
        load.wait()

    def gain_block(step):
        later = pick(order, z, step)
        ag_copy(later, x, c, ag_send.at[later, 2], across).wait_recv()
        for way in (1, -1):
            @pl.when((jnp.where(later < z, 1, -1) == way) & (z + way >= 0) & (z + way < n))
            def _():
                line_copy(later, way).start()

        for copy in spread(later):
            copy.start()

    gain_block(1)

    @pl.when(inner)
    def _():
        gain_block(2)

    def experts(j, carry):
        b = pick(order, z, j)

        ag_copy(b, 1 - x, c, ag_fwd.at[b], sibling).wait_recv()
        forward(b).start()
        for xx in (x, 1 - x):
            ag_copy(b, xx, 1 - c, ag_fwd.at[b], sibling).wait_recv()
        blocks = [ag[b, xx, cc] for cc in (1 - c, c) for xx in range(2)]
        rows_in = jnp.concatenate([block[:, :width] for block in blocks], axis=0)
        marks = jnp.concatenate([block[:, width:] for block in blocks], axis=0).astype(jnp.float32)
        mark_lane = lanes_of(marks.shape) % (LANES // 2)
        active = []
        for e in range(experts_here):
            gate = jnp.dot(rows_in, w_gate[e], preferred_element_type=jnp.float32)
            up = jnp.dot(rows_in, w_up[e], preferred_element_type=jnp.float32)
            weight = jnp.sum(
                jnp.where(mark_lane == z * experts_here + e, marks, 0.0), axis=1, keepdims=True
            )
            active.append((gate / (1.0 + jnp.exp(-gate)) * up * weight).astype(jnp.bfloat16))
        hidden_rows = jnp.concatenate(active, axis=1)
        down = w_down[...].reshape(experts_here * hidden, width)
        split = 2 * rows
        y_out[b] = jnp.dot(
            hidden_rows[:split], down, preferred_element_type=jnp.float32
        ).astype(jnp.bfloat16)
        y_copy(b).start()
        mine = jnp.dot(hidden_rows[split:], down, preferred_element_type=jnp.float32)
        y_copy(b).wait_recv()
        both = mine + y_in[b].astype(jnp.float32)
        xs[b] = jnp.where(x == 0, both[rows:], both[:rows]).astype(jnp.bfloat16)
        x_copy(b).start()
        s1[b] = jnp.where(x == 0, both[:rows], both[rows:])

        ahead = j + jnp.where(inner, 3, 2)

        @pl.when(ahead < n)
        def _():
            gain_block(ahead)

        @pl.when(j > 0)
        def _():
            settle(pick(order, z, j - 1))

        return carry

    lax.fori_loop(0, n, experts, 0)
    settle(pick(order, z, n - 1))

    total = att[...].astype(jnp.float32) + s1[z]
    for away in range(1, n):
        source = (z + away) % n
        remote(zs.at[source], rz.at[source], rz_send.at[source], rz_recv.at[source], {"sp": source}).wait_recv()
        total = total + rz[source].astype(jnp.float32)
    out[...] = total.astype(jnp.bfloat16)

    for h in range(2):
        p_copy(h).wait_send()
        q_copy(h).wait_send()
    for b in range(n):
        for d in (1, -1):
            @pl.when(((z - b) * d >= 0) & (z + d >= 0) & (z + d < n))
            def _():
                for kind in range(2):
                    kv_copy(b, kind, d).wait_send()
                line_copy(b, d).wait_send()

        for copy in spread(b):
            copy.wait_send()
        forward(b).wait_send()
        y_copy(b).wait_send()
        x_copy(b).wait_send()

        @pl.when(b != z)
        def _():
            z_copy(b).wait_send()


def layer_on_device(
    queries_small, keys_small, values_small, queries_large, keys_large, values_large,
    query_gain_small, key_gain_small, query_gain_large, key_gain_large,
    residual_in, out_weight_small, out_weight_large, norm_gain, routes, route_scores,
    expert_gate, expert_up, expert_down,
):
    n = lax.axis_size("sp")
    tokens = queries_small.shape[0]
    rows, width = residual_in.shape
    experts_here, _, hidden = expert_gate.shape
    grid_rows = n * tokens // GRID_W
    small, large = rotary_tables(grid_rows, HS_SMALL), rotary_tables(grid_rows, HS_LARGE)
    row_tab = jnp.asarray(np.stack([small[0][0], small[0][1], large[0][0], large[0][1]]))
    col_tab = jnp.asarray(np.stack([small[1][0], small[1][1], large[1][0], large[1][1]]))
    gains = [
        gain.reshape(1, -1)
        for gain in (query_gain_small, key_gain_small, query_gain_large, key_gain_large)
    ]
    vmem = pl.BlockSpec(memory_space=pltpu.VMEM)
    anywhere = pl.BlockSpec(memory_space=pl.ANY)
    bf, f32 = jnp.bfloat16, jnp.float32
    dma = pltpu.SemaphoreType.DMA
    scratch = [
        pltpu.VMEM((n, 2, 2, tokens, LANES), bf),
        pltpu.VMEM((3, 2 * tokens, LANES), bf),
        pltpu.VMEM((3, 2 * tokens, LANES), f32),
        pltpu.VMEM((3, 2 * tokens, LANES), f32),
        pltpu.VMEM((3, 2 * tokens, LANES), f32),
        pltpu.VMEM((tokens, 4 * LANES), bf),
        pltpu.VMEM((2 * out_weight_small.shape[0], width), bf),
        pltpu.VMEM(expert_gate.shape, bf),
        pltpu.VMEM(expert_up.shape, bf),
        pltpu.VMEM(expert_down.shape, bf),
        pltpu.VMEM((2, 2 * rows, width // 2), bf),
        pltpu.VMEM((2, 2 * rows, width // 2), bf),
        pltpu.VMEM((2, rows, width // 2), bf),
        pltpu.VMEM((2, rows, width // 2), bf),
        pltpu.VMEM((rows, width), bf),
        pltpu.VMEM((n, 2, 2, rows, width + LANES), bf),
        pltpu.VMEM((n, 2 * rows, width), bf),
        pltpu.VMEM((n, 2 * rows, width), bf),
        pltpu.VMEM((n, rows, width), f32),
        pltpu.VMEM((n, rows, width), bf),
        pltpu.VMEM((n, rows, width), bf),
        pltpu.VMEM((n, rows, width), bf),
        pltpu.VMEM((n, rows, width), bf),
        dma((5,)),
        dma((n, 2, 2)), dma((n, 2)),
        dma((2, 2)), dma((2, 2)),
        dma((n, 4)), dma((n,)), dma((n, 2, 2)),
        dma((n,)), dma((n,)),
        dma((n,)), dma((n,)),
        dma((n,)), dma((n,)),
    ]
    return pl.pallas_call(
        functools.partial(layer_kernel, n),
        out_shape=jax.ShapeDtypeStruct((rows, width), bf),
        in_specs=[vmem] * 16 + [anywhere] * 5,
        out_specs=vmem,
        scratch_shapes=scratch,
        compiler_params=pltpu.CompilerParams(
            collective_id=0, has_side_effects=True, vmem_limit_bytes=60 * 1024 * 1024
        ),
    )(
        queries_small, keys_small, values_small, queries_large, keys_large, values_large,
        *gains, row_tab, col_tab, residual_in, norm_gain.reshape(1, width), routes.T, route_scores.T,
        out_weight_small, out_weight_large, expert_gate, expert_up, expert_down,
    )


def choose(mesh, *arrays):
    sp_count, tp_count = mesh.shape["sp"], mesh.shape["tp"]
    rows, top_count = arrays[14].shape
    experts_here = arrays[16].shape[0]
    expert_count = experts_here * sp_count
    capacity = max(2, (2 * top_count * rows + expert_count - 1) // expert_count)
    tokens = arrays[0].shape[0]
    fits = (
        tp_count == 4
        and sp_count > 1
        and expert_count <= LANES // 2
        and tokens == tp_count * rows
        and tokens % GRID_W == 0
        and arrays[1].shape[1] == LANES
        and arrays[4].shape[1] == LANES
        and arrays[0].shape[1] == 2 * LANES
        and arrays[3].shape[1] == 2 * LANES
    )
    if fits and experts_here * capacity >= rows:
        return layer_on_device(*arrays)
    return on_device(*arrays)


def solution(mesh):
    in_specs = (
        P(("grp", "sp"), "tp"),
        P(("grp", "sp"), "tp"),
        P(("grp", "sp"), "tp"),
        P(("grp", "sp"), "tp"),
        P(("grp", "sp"), "tp"),
        P(("grp", "sp"), "tp"),
        P("grp"),
        P("grp"),
        P("grp"),
        P("grp"),
        P(("grp", "sp", "tp"), None),
        P("tp", None),
        P("tp", None),
        P(),
        P(("grp", "sp", "tp"), None),
        P(("grp", "sp", "tp"), None),
        P("sp", None, "tp"),
        P("sp", None, "tp"),
        P("sp", "tp", None),
    )
    out_specs = P(("grp", "sp", "tp"), None)
    return jax.shard_map(
        functools.partial(choose, mesh), mesh=mesh, in_specs=in_specs, out_specs=out_specs, check_vma=False
    )
```
